128 devices in a mesh: kv: 16 (over z, x), tp: 8 (over y, core).
Axes of the slice: x: 4, y: 4, z: 4, core: 2. Of those that a mesh axis runs over, the one named last changes fastest.
Arguments:
- tokens: bfloat16 [32768, 2048], P('kv'), may hold values from -6 to 6
- norm_gain: bfloat16 [2048], replicated, may hold values from 0.099609375 to 1.8984375
- query_weight: bfloat16 [2048, 1024], P(None, 'tp'), may hold values from -0.125 to 0.125
- cmp_key_weight: bfloat16 [2048, 512], P(None, 'tp'), may hold values from -0.125 to 0.125
- cmp_value_weight: bfloat16 [2048, 512], P(None, 'tp'), may hold values from -0.125 to 0.125
- sel_key_weight: bfloat16 [2048, 512], P(None, 'tp'), may hold values from -0.125 to 0.125
- sel_value_weight: bfloat16 [2048, 512], P(None, 'tp'), may hold values from -0.125 to 0.125
- branch_weight: bfloat16 [2, 2048, 16], replicated, may hold values from -0.125 to 0.125
- key_embed: bfloat16 [8, 32, 64], P('tp'), may hold values from -3 to 3
- key_inner: bfloat16 [8, 2048, 64], P('tp'), may hold values from -0.125 to 0.125
- key_outer: bfloat16 [8, 64, 64], P('tp'), may hold values from -0.75 to 0.75
- value_embed: bfloat16 [8, 32, 64], P('tp'), may hold values from -3 to 3
- value_inner: bfloat16 [8, 2048, 64], P('tp'), may hold values from -0.125 to 0.125
- value_outer: bfloat16 [8, 64, 64], P('tp'), may hold values from -0.75 to 0.75
- out_weight: bfloat16 [1024, 2048], replicated, may hold values from -0.1875 to 0.1875
- chosen: int32 [8, 256, 8], P('tp'), may hold values from 0 to 511, as said below
Outputs:
- attended: bfloat16 [32768, 2048], P(('kv', 'tp'))
The draws below stay inside these ranges and needn't reach their ends.
Inputs may be any that keep to these rules, and one draw needn't show every extreme that they name: `chosen`: each entry is the index of a block of 64 positions in the whole sequence. For every key head and query block, its 8 entries lie in 8 different aligned spans of 2048 positions (at most one from any span), and none lies inside the query block's own positions.
All inputs are finite; a program needn't handle non-finite values.
Results may differ from the reference program's by a relative error of at most 0.0075.
Values may be sent and summed in bfloat16 or wider, within the bound.
A program may use at most 128 MiB of HBM per device.

```python
import jax
import jax.numpy as jnp
from jax import lax

D = 2048
HEADS = 16
KV_HEADS = 8
HEAD_DIM = 64
CMP_BLOCK = 32
SEL_BLOCK = 64
Q_BLOCK = 128
FAR_PICKS = 8
TOK_DEV = 2048
SEQ = 32768


def draw_chosen(key, part):
    interval_limits = SEQ // TOK_DEV
    per_span = TOK_DEV // Q_BLOCK
    span_blocks = TOK_DEV // SEL_BLOCK
    own_blocks = Q_BLOCK // SEL_BLOCK
    query_blocks = SEQ // Q_BLOCK
    key_noise, key_inner, key_shift = jax.random.split(key, 3)
    diagonal_group = jnp.arange(query_blocks, dtype=jnp.int32) // per_span
    local_index = jnp.arange(query_blocks, dtype=jnp.int32) % per_span
    eligible_group = jnp.arange(interval_limits, dtype=jnp.int32)
    jitter_perturbation = jax.random.randint(key_noise, (KV_HEADS, query_blocks, interval_limits), 0, 2 ** 16)
    preference_increment = jnp.where(eligible_group[None, :] <= diagonal_group[:, None], 2 ** 24, 0)
    preference_increment = preference_increment + jnp.where(eligible_group[None, :] == diagonal_group[:, None] - 1, 2 ** 26, 0)
    preference_increment = preference_increment + jnp.where(eligible_group[None, :] == diagonal_group[:, None] - interval_limits // 2, 2 ** 26, 0)
    preference_increment = preference_increment + jnp.where(eligible_group[None, :] == 0, 2 ** 25, 0)
    group_relevance = jitter_perturbation * interval_limits + eligible_group[None, None, :] + preference_increment[None]
    _, picked = lax.top_k(group_relevance, FAR_PICKS)
    inside = jax.random.randint(key_inner, (KV_HEADS, query_blocks, FAR_PICKS), 0, span_blocks)
    offset = jax.random.randint(key_shift, (KV_HEADS, query_blocks, FAR_PICKS), 0, span_blocks - own_blocks)
    shifted = (local_index[None, :, None] * own_blocks + own_blocks + offset) % span_blocks
    within = jnp.where(picked == diagonal_group[None, :, None], shifted, inside)
    return (picked * span_blocks + within).astype(jnp.int32)


def block_scale(rng, dims, pieces, smallest, top_value):
    def one(axis_at, blocks):
        draws = jax.random.uniform(jax.random.fold_in(jax.random.fold_in(rng, 6), axis_at), (blocks,), jnp.float32, smallest / len(pieces), top_value / len(pieces))
        return jnp.repeat(jnp.exp(draws), dims[axis_at] // blocks).reshape((-1,) + (1,) * (len(dims) - axis_at - 1))

    factor_of = one(*pieces[0])
    for cut in pieces[1:]:
        factor_of = factor_of * one(*cut)
    return factor_of


def bell_draw(own_key, shape, scale, bound, cuts=(), kind=jnp.bfloat16):
    level = block_scale(own_key, shape, cuts, -0.22, 0.18) if cuts else 1.0
    result = jax.random.normal(own_key, shape, jnp.float32) * scale * level
    return jnp.minimum(jnp.maximum(result, -bound), bound).astype(kind)


def setup_inputs(seed: int = 0) -> dict:
    splits = jax.random.split(jax.random.key(seed), 17)
    return {
        "tokens": bell_draw(splits[0], (SEQ, D), 1.0, 6.0, ((0, 16),)),
        "norm_gain": jnp.clip(1.0 + 0.18 * jax.random.normal(splits[1], (D,), jnp.float32), 0.099609375, 1.8984375).astype(jnp.bfloat16),
        "query_weight": bell_draw(splits[2], (D, HEADS * HEAD_DIM), D ** -0.5, 0.125, ((1, 8),)),
        "cmp_key_weight": bell_draw(splits[3], (D, KV_HEADS * HEAD_DIM), D ** -0.5, 0.125, ((1, 8),)),
        "cmp_value_weight": bell_draw(splits[4], (D, KV_HEADS * HEAD_DIM), D ** -0.5, 0.125, ((1, 8),)),
        "sel_key_weight": bell_draw(splits[5], (D, KV_HEADS * HEAD_DIM), D ** -0.5, 0.125, ((1, 8),)),
        "sel_value_weight": bell_draw(splits[6], (D, KV_HEADS * HEAD_DIM), D ** -0.5, 0.125, ((1, 8),)),
        "branch_weight": bell_draw(splits[7], (2, D, HEADS), D ** -0.5, 0.125),
        "key_embed": bell_draw(splits[8], (KV_HEADS, CMP_BLOCK, HEAD_DIM), 0.5, 3.0, ((0, 8),)),
        "key_inner": bell_draw(splits[9], (KV_HEADS, CMP_BLOCK * HEAD_DIM, HEAD_DIM), (CMP_BLOCK * HEAD_DIM) ** -0.5, 0.125, ((0, 8),)),
        "key_outer": bell_draw(splits[10], (KV_HEADS, HEAD_DIM, HEAD_DIM), HEAD_DIM ** -0.5, 0.75, ((0, 8),)),
        "value_embed": bell_draw(splits[11], (KV_HEADS, CMP_BLOCK, HEAD_DIM), 0.5, 3.0, ((0, 8),)),
        "value_inner": bell_draw(splits[12], (KV_HEADS, CMP_BLOCK * HEAD_DIM, HEAD_DIM), (CMP_BLOCK * HEAD_DIM) ** -0.5, 0.125, ((0, 8),)),
        "value_outer": bell_draw(splits[13], (KV_HEADS, HEAD_DIM, HEAD_DIM), HEAD_DIM ** -0.5, 0.75, ((0, 8),)),
        "out_weight": bell_draw(splits[14], (HEADS * HEAD_DIM, D), (HEADS * HEAD_DIM) ** -0.5, 0.1875),
        "chosen": draw_chosen(jax.random.fold_in(splits[16], 71), 0),
    }


ROPE_BASE = 10000.0
norm_eps = 1e-06
masked_score = -1000000000.0

def rotate(values_in, positions):
    half_dim = values_in.shape[-1] // 2
    inverse = ROPE_BASE ** (-jnp.arange(half_dim, dtype=jnp.float32) / half_dim)
    rotary_phases = positions.astype(jnp.float32)[:, None] * inverse[None, :]
    cosine = jnp.cos(rotary_phases)[:, None, :]
    sine = jnp.sin(rotary_phases)[:, None, :]
    first_half = values_in[..., :half_dim]
    second_half = values_in[..., half_dim:]
    return jnp.concatenate([first_half * cosine - second_half * sine, second_half * cosine + first_half * sine], axis=-1)

def summarize(raw_rows, embed, inner, outer):
    block_count = raw_rows.shape[0] // CMP_BLOCK
    blocked = raw_rows.reshape(block_count, CMP_BLOCK, KV_HEADS, HEAD_DIM).transpose(2, 0, 1, 3).astype(jnp.float32)
    blocked = (blocked + embed.astype(jnp.float32)[:, None]).astype(jnp.bfloat16)
    blocked = blocked.reshape(KV_HEADS, block_count, CMP_BLOCK * HEAD_DIM)
    hidden = jax.nn.gelu(jnp.einsum('knc,kce->kne', blocked.astype(jnp.float32), inner.astype(jnp.float32))).astype(jnp.bfloat16)
    return jnp.einsum('kne,kef->knf', hidden.astype(jnp.float32), outer.astype(jnp.float32)).astype(jnp.bfloat16)

def reference(tokens, norm_gain, query_weight, cmp_key_weight, cmp_value_weight, sel_key_weight, sel_value_weight, branch_weight, key_embed, key_inner, key_outer, value_embed, value_inner, value_outer, out_weight, chosen):
    length = tokens.shape[0]
    group_size = HEADS // KV_HEADS
    positions = jnp.arange(length, dtype=jnp.int32)
    scale = HEAD_DIM ** (-0.5)
    expanded_mask = tokens.astype(jnp.float32)
    normed = (expanded_mask * lax.rsqrt(lax.optimization_barrier(jnp.mean(expanded_mask * expanded_mask, axis=-1, keepdims=True)) + norm_eps) * norm_gain.astype(jnp.float32)).astype(jnp.bfloat16)

    def project(weight_in):
        return jnp.dot(normed, weight_in, preferred_element_type=jnp.float32)
    query = project(query_weight).reshape(length, HEADS, HEAD_DIM)
    q_plain = query.astype(jnp.bfloat16)
    q_turn = rotate(query, positions).astype(jnp.bfloat16)
    cmp_key = project(cmp_key_weight).astype(jnp.bfloat16).reshape(length, KV_HEADS, HEAD_DIM)
    cmp_value = project(cmp_value_weight).astype(jnp.bfloat16).reshape(length, KV_HEADS, HEAD_DIM)
    sel_key = rotate(project(sel_key_weight).reshape(length, KV_HEADS, HEAD_DIM), positions).astype(jnp.bfloat16)
    selected_value = project(sel_value_weight).astype(jnp.bfloat16).reshape(length, KV_HEADS, HEAD_DIM)
    gate_cmp = jax.nn.sigmoid(project(branch_weight[0]))
    gate_sel = jax.nn.sigmoid(project(branch_weight[1]))
    summary_key = summarize(cmp_key, key_embed, key_inner, key_outer)
    summary_value = summarize(cmp_value, value_embed, value_inner, value_outer)
    summary_count = summary_key.shape[1]
    block_end = (jnp.arange(summary_count, dtype=jnp.int32) + 1) * CMP_BLOCK - 1

    def compress_head(packed_rows):
        head_query, head_keys, head_values = packed_rows
        scores = jnp.einsum('tgd,cd->tgc', head_query.astype(jnp.float32), head_keys.astype(jnp.float32)) * scale
        allowed_keys = (block_end[None, :] <= positions[:, None])[:, None, :]
        probs = jax.nn.softmax(jnp.where(allowed_keys, scores, masked_score), axis=-1) * allowed_keys.astype(jnp.float32)
        return jnp.einsum('tgc,cd->tgd', probs.astype(jnp.bfloat16).astype(jnp.float32), head_values.astype(jnp.float32))
    q_group = q_plain.reshape(length, KV_HEADS, group_size, HEAD_DIM).transpose(1, 0, 2, 3)
    out_cmp = lax.map(compress_head, (q_group, summary_key, summary_value))
    out_cmp = out_cmp.transpose(1, 0, 2, 3).reshape(length, HEADS, HEAD_DIM)
    query_blocks = length // Q_BLOCK
    block_pos = jnp.arange(query_blocks, dtype=jnp.int32)[:, None] * Q_BLOCK + jnp.arange(Q_BLOCK, dtype=jnp.int32)[None, :]

    def select_head(packed_rows):
        head_query, head_keys, head_values, head_picks = packed_rows
        far_keys = head_keys.reshape(-1, SEL_BLOCK, HEAD_DIM)[head_picks].reshape(query_blocks, FAR_PICKS * SEL_BLOCK, HEAD_DIM)
        far_values = head_values.reshape(-1, SEL_BLOCK, HEAD_DIM)[head_picks].reshape(query_blocks, FAR_PICKS * SEL_BLOCK, HEAD_DIM)
        all_keys = jnp.concatenate([head_keys.reshape(query_blocks, Q_BLOCK, HEAD_DIM), far_keys], axis=1)
        all_values = jnp.concatenate([head_values.reshape(query_blocks, Q_BLOCK, HEAD_DIM), far_values], axis=1)
        far_pos = (head_picks[:, :, None] * SEL_BLOCK + jnp.arange(SEL_BLOCK, dtype=jnp.int32)[None, None, :]).reshape(query_blocks, -1)
        key_pos = jnp.concatenate([block_pos, far_pos], axis=1)
        allowed_keys = key_pos[:, None, None, :] <= block_pos[:, :, None, None]
        scores = jnp.einsum('nqgd,nmd->nqgm', head_query.astype(jnp.float32), all_keys.astype(jnp.float32)) * scale
        probs = jax.nn.softmax(jnp.where(allowed_keys, scores, masked_score), axis=-1)
        return jnp.einsum('nqgm,nmd->nqgd', probs.astype(jnp.bfloat16).astype(jnp.float32), all_values.astype(jnp.float32))
    q_sel = q_turn.reshape(query_blocks, Q_BLOCK, KV_HEADS, group_size, HEAD_DIM).transpose(2, 0, 1, 3, 4)
    out_sel = lax.map(select_head, (q_sel, sel_key.transpose(1, 0, 2), selected_value.transpose(1, 0, 2), chosen.astype(jnp.int32)))
    out_sel = out_sel.transpose(1, 2, 0, 3, 4).reshape(length, HEADS, HEAD_DIM)
    mixed = (gate_cmp[..., None] * out_cmp + gate_sel[..., None] * out_sel).reshape(length, HEADS * HEAD_DIM).astype(jnp.bfloat16)
    return jnp.dot(mixed, out_weight, preferred_element_type=jnp.float32).astype(jnp.bfloat16)
```

```python
import functools

import jax
import jax.numpy as jnp
import numpy as np
from jax import lax
from jax.experimental import pallas as pl
from jax.experimental.pallas import tpu as pltpu
from jax.sharding import PartitionSpec as P

D = 2048
HD = 64
CMP = 32
SEL = 64
QB = 128
TOK = 2048
NQ = TOK // QB
NB = TOK // SEL
EPS = 1e-06
NEG = -1e30
FLOOR = -1e20
TILE = 512
MESH = pl.DeviceIdType.MESH
NT = (((1,), (1,)), ((), ()))
ORDER = ((2, 0), (2, 1), (1, 0), (3, 0), (1, 1), (3, 1), (0, 1), (0, 0))


def angle_tables():
    lane = np.arange(128)
    freq = 10000.0 ** (-(lane % 32) / 32.0)
    sign = np.where(lane % 64 < 32, -1.0, 1.0)
    coarse = np.arange(512)[:, None] * 64.0 * freq
    fine = np.arange(64)[:, None] * freq
    as32 = lambda t: np.asarray(t, np.float32)
    return as32(np.cos(coarse)), as32(np.sin(coarse)), as32(np.cos(fine)), as32(np.sin(fine)), as32(sign[None])


def lanes(shape):
    return lax.broadcasted_iota(jnp.int32, shape, 1)


def gelu(x):
    return 0.5 * x * (1.0 + jnp.tanh(0.7978845608028654 * (x + 0.044715 * (x * x * x))))


def project_kernel(
    tok_ref, gain_ref, wq_ref, wck_ref, wcv_ref, wsk_ref, wsv_ref, bw_ref, ke_ref, ki_ref, ko_ref,
    ve_ref, vi_ref, vo_ref, cc_ref, cs_ref, fc_ref, fs_ref, sg_ref,
    kv_ref, qs_ref, qc_ref, g_ref, sum_ref,
    w_ref, raw_ref,
):
    step = pl.program_id(0)
    tp = lax.axis_index("tp")
    kv = lax.axis_index("kv")

    @pl.when(step == 0)
    def _():
        w_ref[0:64, :] = wsk_ref[...]
        w_ref[64:128, :] = wsv_ref[...]
        w_ref[128:192, :] = wck_ref[...]
        w_ref[192:256, :] = wcv_ref[...]
        w_ref[256:384, :] = wq_ref[...].T
        row = lax.broadcasted_iota(jnp.int32, (128, 16), 0)
        col = lax.broadcasted_iota(jnp.int32, (128, 16), 1)
        e0 = jnp.where((row < 2) & (col == 2 * tp + row), 1.0, 0.0).astype(jnp.bfloat16)
        e1 = jnp.where((row >= 2) & (row < 4) & (col == 2 * tp + row - 2), 1.0, 0.0).astype(jnp.bfloat16)
        picked = jnp.dot(e0, bw_ref[0], preferred_element_type=jnp.float32)
        picked += jnp.dot(e1, bw_ref[1], preferred_element_type=jnp.float32)
        w_ref[384:512, :] = picked.astype(jnp.bfloat16)

    x = tok_ref[...].astype(jnp.float32)
    inv = lax.rsqrt(jnp.mean(x * x, axis=1, keepdims=True) + EPS)
    normed = (x * inv * gain_ref[...].astype(jnp.float32)).astype(jnp.bfloat16)
    proj = lax.dot_general(normed, w_ref[...], NT, preferred_element_type=jnp.float32)
    base = kv * 32 + step * (TILE // 64)
    cosine, sine = [], []
    for u in range(TILE // 64):
        cc = cc_ref[pl.ds(base + u, 1), :]
        cs = cs_ref[pl.ds(base + u, 1), :]
        cosine.append(cc * fc_ref[...] - cs * fs_ref[...])
        sine.append((cs * fc_ref[...] + cc * fs_ref[...]) * sg_ref[...])
    cosine = jnp.concatenate(cosine, axis=0)
    sine = jnp.concatenate(sine, axis=0)
    lane = lanes((TILE, 128))
    front = (lane % 64) < 32
    low = lane < 64

    def turn(v):
        other = jnp.where(front, pltpu.roll(v, 96, 1), pltpu.roll(v, 32, 1))
        return v * cosine + other * sine

    sel = proj[:, 0:128]
    kv_ref[...] = jnp.where(low, turn(sel), sel).astype(jnp.bfloat16)
    raw = proj[:, 128:256].astype(jnp.bfloat16).astype(jnp.float32)
    embed = jnp.concatenate([ke_ref[...], ve_ref[...]], axis=1).astype(jnp.float32)
    raw = raw + jnp.concatenate([embed] * (TILE // CMP), axis=0)
    raw_ref[pl.ds(pl.multiple_of(step * TILE, TILE), TILE), :] = raw.astype(jnp.bfloat16).astype(jnp.float32)
    q = proj[:, 256:384]
    for ref, val in ((qc_ref, q), (qs_ref, turn(q))):
        val = val.astype(jnp.bfloat16).astype(jnp.float32) * 0.125
        ref[0] = jnp.where(low, val, 0.0).astype(jnp.bfloat16)
        ref[1] = jnp.where(low, pltpu.roll(val, 64, 1), 0.0).astype(jnp.bfloat16)
    g_ref[...] = 1.0 / (1.0 + jnp.exp(-proj[:, 384:512]))

    @pl.when(step == TOK // TILE - 1)
    def _():
        keys, values = [], []
        low64 = lanes((64, 128)) < 64
        for r in range(0, CMP, 2):
            one = raw_ref[pl.ds(r, 64, stride=CMP), :]
            two = raw_ref[pl.ds(r + 1, 64, stride=CMP), :]
            keys.append(jnp.where(low64, one, pltpu.roll(two, 64, 1)).astype(jnp.bfloat16))
            values.append(jnp.where(low64, pltpu.roll(one, 64, 1), two).astype(jnp.bfloat16))
        parts = []
        for rows, inner, outer in ((keys, ki_ref, ko_ref), (values, vi_ref, vo_ref)):
            flat = jnp.concatenate(rows, axis=1)
            hidden = lax.dot_general(flat, inner[...], NT, preferred_element_type=jnp.float32)
            hidden = gelu(hidden).astype(jnp.bfloat16)
            parts.append(jnp.dot(hidden, outer[...], preferred_element_type=jnp.float32))
        sum_ref[...] = jnp.concatenate(parts, axis=1).astype(jnp.bfloat16)


def run_project(tokens, gain, wq, wck, wcv, wsk, wsv, bw, ke, ki, ko, ve, vi, vo):
    cc, cs, fc, fs, sg = angle_tables()
    whole = lambda shape: pl.BlockSpec(shape, lambda i: (0,) * len(shape))
    ops = [gain, wq, wck, wcv, wsk, wsv, bw, ke, ki, ko, ve, vi, vo] + [jnp.asarray(t) for t in (cc, cs, fc, fs, sg)]
    return pl.pallas_call(
        project_kernel,
        grid=(TOK // TILE,),
        in_specs=[pl.BlockSpec((TILE, D), lambda i: (i, 0))] + [whole(o.shape) for o in ops],
        out_specs=[
            pl.BlockSpec((TILE, 128), lambda i: (i, 0)),
            pl.BlockSpec((2, TILE, 128), lambda i: (0, i, 0)),
            pl.BlockSpec((2, TILE, 128), lambda i: (0, i, 0)),
            pl.BlockSpec((TILE, 128), lambda i: (i, 0)),
            whole((64, 128)),
        ],
        out_shape=[
            jax.ShapeDtypeStruct((TOK, 128), jnp.bfloat16),
            jax.ShapeDtypeStruct((2, TOK, 128), jnp.bfloat16),
            jax.ShapeDtypeStruct((2, TOK, 128), jnp.bfloat16),
            jax.ShapeDtypeStruct((TOK, 128), jnp.float32),
            jax.ShapeDtypeStruct((64, 128), jnp.bfloat16),
        ],
        scratch_shapes=[pltpu.VMEM((512, D), jnp.bfloat16), pltpu.VMEM((TOK, 128), jnp.float32)],
        compiler_params=pltpu.CompilerParams(vmem_limit_bytes=48 << 20),
        name="project",
    )(tokens, *ops)


def attend_kernel(
    want_ref, bias_ref, kv_ref, summ_ref, qs_ref, qc_ref, g_ref,
    out_ref,
    full1, full2, full3, inb, outb, fwd, sums, acc, mrow, ocmp, mix, hr,
    a_send, a_recv, af_send, af_recv, s_send, s_recv, b_send, b_recv, f_send, f_recv, t_send, t_recv,
):
    full = (kv_ref, full1, full2, full3)
    tp = lax.axis_index("tp")
    kv = lax.axis_index("kv")
    core = lax.rem(tp, 2)
    yy = tp // 2
    zz = kv // 4
    xx = lax.rem(kv, 4)
    sa = 4 - 3 * core
    sb = 1 + 3 * core
    aa = zz * (1 - core) + xx * core
    bb = xx * (1 - core) + zz * core

    def at(r, s):
        return lax.rem(aa + r, 4) * sa + lax.rem(bb + s, 4) * sb

    def tp_at(dy, dc):
        return 2 * lax.rem(yy + dy, 4) + (core + dc - 2 * core * dc)

    def near(r, s):
        return {"kv": at(r, s), "tp": tp}

    barrier = pltpu.get_barrier_semaphore()
    peers = [near(r, 0) for r in (1, 2, 3)] + [near(0, s) for s in (1, 2, 3)]
    peers += [{"kv": kv, "tp": tp_at(*o)} for o in ORDER[:-1]]
    for peer in peers:
        pl.semaphore_signal(barrier, inc=1, device_id=peer, device_id_type=MESH)
    pl.semaphore_wait(barrier, len(peers))

    def remote(src, dst, ssem, rsem, dev):
        return pltpu.make_async_remote_copy(
            src_ref=src, dst_ref=dst, send_sem=ssem, recv_sem=rsem, device_id=dev, device_id_type=MESH
        )

    started = []

    def go(copy):
        copy.start()
        started.append(copy)

    sums[0, 0] = summ_ref[...]
    for r in (1, 2, 3):
        go(remote(summ_ref, sums.at[0, 4 - r], s_send.at[r - 1], s_recv.at[3 - r], near(r, 0)))
    half = NB // 2
    for h in (0, 1):
        for r, slot, part in ((1, 3, h), (3, 1, 1 - h)):
            rows = pl.ds(part * half, half)
            i = (slot // 2) * 2 + part
            go(remote(kv_ref.at[rows], full[slot].at[rows], a_send.at[i], a_recv.at[i], near(r, 0)))

    def a_wait(slot, part):
        rows = pl.ds(part * half, half)
        i = (slot // 2) * 2 + part
        remote(kv_ref.at[rows], full[slot].at[rows], a_send.at[i], a_recv.at[i], near(1, 0)).wait_recv()

    def a_forward(slot, part, r, i):
        rows = pl.ds(part * half, half)
        go(remote(full[slot].at[rows], full[2].at[rows], af_send.at[i], af_recv.at[i], near(r, 0)))

    def af_wait(i):
        rows = pl.ds(i * half, half)
        remote(full[0].at[rows], full[2].at[rows], af_send.at[i], af_recv.at[i], near(1, 0)).wait_recv()

    def order_of(c):
        return [tp_at(*o) for o in ORDER][c]

    def q_of(i):
        c = i // 2
        dest = 0
        for k in range(8):
            dest = dest + jnp.where(c == k, tp_at(*ORDER[k]), 0)
        return dest * 2 + lax.rem(i, 2)

    def select(r):
        span = at(r, 0)
        dests = [at(0, s) for s in range(4)]

        def body(i, _):
            q = q_of(i)
            for s in range(4):
                blk = want_ref[span * 256 + dests[s] * 16 + q]
                val = full[r][blk]
                if s == 0:
                    inb[r, 0, i] = val
                else:
                    outb[r, s - 1, i] = val
            return 0

        lax.fori_loop(0, NQ, body, 0)

    def b_start(r):
        go(remote(outb.at[r, 1, pl.ds(0, 8)], fwd.at[r, 0], f_send.at[r, 0], f_recv.at[r, 0], near(0, 1)))
        go(remote(outb.at[r, 1, pl.ds(8, 8)], fwd.at[r, 1], f_send.at[r, 1], f_recv.at[r, 1], near(0, 3)))
        go(remote(outb.at[r, 0], inb.at[r, 3], b_send.at[r, 0], b_recv.at[r, 0], near(0, 1)))
        go(remote(outb.at[r, 2], inb.at[r, 1], b_send.at[r, 1], b_recv.at[r, 1], near(0, 3)))

    def b_forward(r):
        for k, s in ((0, 1), (1, 3)):
            remote(outb.at[r, 1, pl.ds(8 * k, 8)], fwd.at[r, k], f_send.at[r, k], f_recv.at[r, k], near(0, 1)).wait_recv()
            go(remote(fwd.at[r, k], inb.at[r, 2, pl.ds(8 * k, 8)], b_send.at[r, 2 + k], b_recv.at[r, 2 + k], near(0, s)))

    def b_wait(r):
        remote(outb.at[r, 0], inb.at[r, 3], b_send.at[r, 0], b_recv.at[r, 0], near(0, 1)).wait_recv()
        remote(outb.at[r, 2], inb.at[r, 1], b_send.at[r, 1], b_recv.at[r, 1], near(0, 1)).wait_recv()
        for k in (0, 1):
            remote(fwd.at[r, k], inb.at[r, 2, pl.ds(8 * k, 8)], b_send.at[r, 2 + k], b_recv.at[r, 2 + k], near(0, 1)).wait_recv()

    def with_ones(keys):
        return jnp.where(lanes(keys.shape) < HD, jnp.ones_like(keys), keys)

    def scores(q2, keys):
        return lax.dot_general(q2, keys, NT, preferred_element_type=jnp.float32)

    def spread(col):
        return jnp.broadcast_to(col, (2 * QB, 128))

    def weigh(s, m, keys):
        p = jnp.concatenate([jnp.exp(s[:, k:k + 128] - m) for k in range(0, s.shape[1], 128)], axis=1)
        return jnp.dot(p.astype(jnp.bfloat16), with_ones(keys), preferred_element_type=jnp.float32)

    def stacked(ref, q):
        rows = pl.ds(pl.multiple_of(q * QB, QB), QB)
        return jnp.concatenate([ref[0, rows, :], ref[1, rows, :]], axis=0)

    def own_block(i, _):
        q = q_of(i)
        keys = kv_ref[pl.ds(2 * q, 2)].reshape(QB, 128)
        s = scores(stacked(qs_ref, q), keys)
        row = lax.rem(lax.broadcasted_iota(jnp.int32, s.shape, 0), QB)
        s = jnp.where(lanes(s.shape) <= row, s, NEG)
        m = spread(jnp.max(s, axis=1, keepdims=True))
        mrow[i] = m
        acc[i] = weigh(s, m, keys)
        return 0

    def far_step(i, r):
        q = q_of(i)
        keys = inb[r, :, i].reshape(4 * SEL, 128)
        s = scores(stacked(qs_ref, q), keys) + bias_ref[pl.ds(q, 1), r * 256:(r + 1) * 256]
        old = mrow[i]
        m = jnp.maximum(old, spread(jnp.max(s, axis=1, keepdims=True)))
        return m, acc[i] * jnp.exp(old - m) + weigh(s, m, keys)

    def far(r):
        def body(i, _):
            m, a = far_step(i, r)
            mrow[i] = m
            acc[i] = a
            return 0

        lax.fori_loop(0, NQ, body, 0)

    def heads_of(top, bottom):
        low = lanes((QB, 128)) < HD
        num = jnp.where(low, pltpu.roll(top, HD, 1), bottom)
        den = jnp.where(low, top, pltpu.roll(bottom, HD, 1))
        return num, den

    def compressed(i, _):
        q = q_of(i)
        q2 = stacked(qc_ref, q)
        pos = kv * TOK + q * QB + lax.rem(lax.broadcasted_iota(jnp.int32, (2 * QB, 128), 0), QB)
        m = jnp.full((2 * QB, 128), FLOOR, jnp.float32)
        ss = []
        for s in range(4):
            keys = sums[s].reshape(4 * 64, 128)
            sc = scores(q2, keys)
            lane = lanes((1, 256))
            r = lane // 64
            span = lax.rem(aa + r, 4) * sa + lax.rem(bb + s, 4) * sb
            end = span * TOK + (lax.rem(lane, 64) + 1) * CMP - 1
            sc = jnp.concatenate(
                [jnp.where(end[:, k:k + 128] <= pos, sc[:, k:k + 128], NEG) for k in (0, 128)], axis=1
            )
            ss.append(sc)
            m = jnp.maximum(m, jnp.maximum(sc[:, :128], sc[:, 128:]))
        m = spread(jnp.maximum(jnp.max(m, axis=1, keepdims=True), FLOOR))
        total = jnp.zeros((2 * QB, 128), jnp.float32)
        for s in range(4):
            total += weigh(ss[s], m, sums[s].reshape(4 * 64, 128))
        num, den = heads_of(total[:QB], total[QB:])
        ocmp[pl.ds(pl.multiple_of(i * QB, QB), QB), :] = jnp.where(den > 0, num / jnp.maximum(den, 1e-30), 0.0)
        return 0

    def finish(i, r):
        q = q_of(i)
        m, a = far_step(i, r)
        num, den = heads_of(a[:QB], a[QB:])
        rows = pl.ds(pl.multiple_of(q * QB, QB), QB)
        g = g_ref[rows, :]
        low = lanes((QB, 128)) < HD
        gc = jnp.where(low, g[:, 0:1], g[:, 1:2])
        gs = jnp.where(low, g[:, 2:3], g[:, 3:4])
        return gc * ocmp[pl.ds(pl.multiple_of(i * QB, QB), QB), :] + gs * (num / den)

    select(0)
    lax.fori_loop(0, NQ, own_block, 0)
    for r in (1, 2, 3):
        remote(summ_ref, sums.at[0, 4 - r], s_send.at[r - 1], s_recv.at[3 - r], near(r, 0)).wait_recv()
    for s in (1, 2, 3):
        go(remote(sums.at[0], sums.at[4 - s], s_send.at[2 + s], s_recv.at[6 - s], near(0, s)))
    b_start(0)
    for s in (1, 2, 3):
        remote(sums.at[0], sums.at[4 - s], s_send.at[2 + s], s_recv.at[6 - s], near(0, s)).wait_recv()
    lax.fori_loop(0, 4, compressed, 0)
    a_wait(3, 0)
    a_forward(3, 0, 1, 0)
    a_wait(1, 1)
    a_forward(1, 1, 3, 1)
    lax.fori_loop(4, 8, compressed, 0)
    b_forward(0)
    lax.fori_loop(8, 12, compressed, 0)
    a_wait(3, 1)
    select(3)
    b_start(3)
    a_wait(1, 0)
    select(1)
    b_start(1)
    lax.fori_loop(12, 16, compressed, 0)
    af_wait(0)
    af_wait(1)
    select(2)
    b_start(2)
    b_wait(0)
    far(0)
    b_forward(3)
    b_forward(1)
    b_wait(3)
    far(3)
    b_forward(2)
    b_wait(1)
    far(1)
    b_wait(2)
    for c in range(8):
        for k in (0, 1):
            mix[c, k * QB:(k + 1) * QB, :] = finish(2 * c + k, 2).astype(jnp.bfloat16)
        if c < 7:
            go(remote(mix.at[c], hr.at[tp], t_send.at[c], t_recv.at[c], {"kv": kv, "tp": order_of(c)}))
        else:
            hr[tp] = mix[7]
    for c in range(7):
        dy, dc = ORDER[c]
        src = tp_at(4 - dy if dy else 0, dc)
        remote(mix.at[c], hr.at[src], t_send.at[c], t_recv.at[c], {"kv": kv, "tp": order_of(c)}).wait_recv()
    for t in range(8):
        out_ref[:, t * 128:(t + 1) * 128] = hr[t]
    for copy in started:
        copy.wait_send()


def run_attend(want, bias, kvrows, summ, qs, qc, g):
    vm = pl.BlockSpec(memory_space=pltpu.VMEM)
    bf = jnp.bfloat16
    dma = pltpu.SemaphoreType.DMA
    return pl.pallas_call(
        attend_kernel,
        in_specs=[pl.BlockSpec(memory_space=pltpu.SMEM)] + [vm] * 6,
        out_specs=vm,
        out_shape=jax.ShapeDtypeStruct((256, 1024), bf),
        scratch_shapes=[
            pltpu.VMEM((NB, SEL, 128), bf),
            pltpu.VMEM((NB, SEL, 128), bf),
            pltpu.VMEM((NB, SEL, 128), bf),
            pltpu.VMEM((4, 4, NQ, SEL, 128), bf),
            pltpu.VMEM((4, 3, NQ, SEL, 128), bf),
            pltpu.VMEM((4, 2, 8, SEL, 128), bf),
            pltpu.VMEM((4, 4, 64, 128), bf),
            pltpu.VMEM((NQ, 2 * QB, 128), jnp.float32),
            pltpu.VMEM((NQ, 2 * QB, 128), jnp.float32),
            pltpu.VMEM((TOK, 128), jnp.float32),
            pltpu.VMEM((8, 256, 128), bf),
            pltpu.VMEM((8, 256, 128), bf),
            dma((4,)), dma((4,)), dma((2,)), dma((2,)), dma((6,)), dma((6,)),
            dma((4, 4)), dma((4, 4)), dma((4, 2)), dma((4, 2)), dma((8,)), dma((8,)),
        ],
        compiler_params=pltpu.CompilerParams(
            collective_id=0, has_side_effects=True, vmem_limit_bytes=56 << 20
        ),
        name="attend",
    )(want, bias, kvrows, summ, qs, qc, g)


def pick_tables(chosen):
    tp = lax.axis_index("tp")
    kv = lax.axis_index("kv")
    core = tp % 2
    sa, sb = 4 - 3 * core, 1 + 3 * core
    aa = jnp.where(core == 0, kv // 4, kv % 4)
    bb = jnp.where(core == 0, kv % 4, kv // 4)
    picks = chosen[0].T
    span = picks // NB
    match = span[None] == jnp.arange(16, dtype=jnp.int32)[:, None, None]
    want = jnp.sum(jnp.where(match, (picks % NB)[None], 0), axis=1).reshape(4096)
    mine = lax.dynamic_slice_in_dim(chosen[0], kv * NQ, NQ, 0)
    col = jnp.arange(1024, dtype=jnp.int32)
    where_from = ((aa + col // 256) % 4) * sa + ((bb + (col // 64) % 4) % 4) * sb
    start = (kv * NQ + jnp.arange(NQ, dtype=jnp.int32)) * (QB // SEL)
    good = (mine // NB)[:, :, None] == where_from[None, None, :]
    good = good & (mine < start[:, None])[:, :, None]
    bias = jnp.where(jnp.any(good, axis=1), 0.0, NEG).astype(jnp.float32)
    return want, bias


def per_device(
    tokens, norm_gain, query_weight, cmp_key_weight, cmp_value_weight, sel_key_weight, sel_value_weight,
    branch_weight, key_embed, key_inner, key_outer, value_embed, value_inner, value_outer, out_weight, chosen,
):
    want, bias = pick_tables(chosen)
    kvrows, qs, qc, g, summ = run_project(
        tokens, norm_gain.reshape(1, D), query_weight, cmp_key_weight.T, cmp_value_weight.T, sel_key_weight.T,
        sel_value_weight.T, branch_weight.transpose(0, 2, 1), key_embed[0], key_inner[0].T, key_outer[0],
        value_embed[0], value_inner[0].T, value_outer[0],
    )
    rows = run_attend(want, bias, kvrows.reshape(NB, SEL, 128), summ, qs, qc, g)
    return jnp.dot(rows, out_weight, preferred_element_type=jnp.float32).astype(jnp.bfloat16)


def solution(mesh):
    placed = (
        P("kv", None), P(), P(None, "tp"), P(None, "tp"), P(None, "tp"), P(None, "tp"), P(None, "tp"), P(),
        P("tp", None, None), P("tp", None, None), P("tp", None, None), P("tp", None, None),
        P("tp", None, None), P("tp", None, None), P(), P("tp", None, None),
    )
    return jax.shard_map(
        per_device, mesh=mesh, in_specs=placed, out_specs=P(("kv", "tp"), None), check_vma=False
    )
```

```python
import jax
import jax.numpy as jnp
import numpy as np
from jax import lax
from jax.experimental import pallas as pl
from jax.experimental.pallas import tpu as pltpu
from jax.sharding import PartitionSpec as P

D = 2048
HD = 64
CMP = 32
SEL = 64
QB = 128
TOK = 2048
NQ = TOK // QB
NB = TOK // SEL
EPS = 1e-06
NEG = -1e30
FLOOR = -1e20
TILE = 512
MESH = pl.DeviceIdType.MESH
NT = (((1,), (1,)), ((), ()))
BF = jnp.bfloat16
F32 = jnp.float32
ORDER = ((2, 0), (2, 1), (1, 0), (3, 0), (1, 1), (3, 1), (0, 1), (0, 0))


def angle_tables():
    lane = np.arange(128)
    freq = 10000.0 ** (-(lane % 32) / 32.0)
    sign = np.where(lane % 64 < 32, -1.0, 1.0)
    coarse = np.arange(512)[:, None] * 64.0 * freq
    fine = np.arange(64)[:, None] * freq
    as32 = lambda t: jnp.asarray(np.asarray(t, np.float32))
    return as32(np.cos(coarse)), as32(np.sin(coarse)), as32(np.cos(fine)), as32(np.sin(fine)), as32(sign[None])


def lanes(shape):
    return lax.broadcasted_iota(jnp.int32, shape, 1)


def rows_of(shape):
    return lax.broadcasted_iota(jnp.int32, shape, 0)


def gelu(x):
    return 0.5 * x * (1.0 + jnp.tanh(0.7978845608028654 * (x + 0.044715 * (x * x * x))))


def kernel(
    tab, gain_ref, ke_ref, ko_ref, ve_ref, vo_ref, fc_ref, fs_ref, sg_ref,
    tok_hbm, wq_hbm, wck_hbm, wcv_hbm, wsk_hbm, wsv_hbm, bw_hbm, ki_hbm, vi_hbm, cc_hbm, cs_hbm, ow_hbm,
    out_hbm,
    tok, wst, w1, wqv, bwv, w2, kiv, viv, ccv, csv, ow, inv_s, cos_s, sin_s, raw, qs, qc, gt,
    kvb, full1, full2, full3, inb, outb, fwd, own, sums, vtc, acc, mrow, ocmp, mix, hr, res,
    l_sem, a_send, a_recv, af_send, af_recv, s_send, s_recv, b_send, b_recv, f_send, f_recv, t_send, t_recv, o_sem,
):
    full = (kvb, full1, full2, full3)
    tp = lax.axis_index("tp")
    kv = lax.axis_index("kv")
    core = lax.rem(tp, 2)
    yy = tp // 2
    zz = kv // 4
    xx = lax.rem(kv, 4)
    sa = 4 - 3 * core
    sb = 1 + 3 * core
    aa = zz * (1 - core) + xx * core
    bb = xx * (1 - core) + zz * core

    def at(r, s):
        return lax.rem(aa + r, 4) * sa + lax.rem(bb + s, 4) * sb

    def tp_at(dy, dc):
        return 2 * lax.rem(yy + dy, 4) + (core + dc - 2 * core * dc)

    def near(r, s):
        return {"kv": at(r, s), "tp": tp}

    local = []

    def fetch(src, dst):
        copy = pltpu.make_async_copy(src, dst, l_sem.at[len(local)])
        copy.start()
        local.append(copy)
        return copy

    w_in = [fetch(h, wst.at[pl.ds(64 * k, 64)]) for k, h in enumerate((wsk_hbm, wsv_hbm, wck_hbm, wcv_hbm))]
    tiles = TOK // TILE

    def tok_in(t):
        return fetch(tok_hbm.at[pl.ds(t * TILE, TILE)], tok.at[pl.ds(t * TILE, TILE)])

    t_in = [tok_in(0)]
    base = pl.ds(pl.multiple_of(kv * 32, 32), 32)
    a_in = [fetch(cc_hbm.at[base], ccv), fetch(cs_hbm.at[base], csv)]
    t_in += [tok_in(1), tok_in(2), tok_in(3)]
    q_in = [fetch(wq_hbm, wqv), fetch(bw_hbm, bwv)]
    i_in = [fetch(ki_hbm, kiv), fetch(vi_hbm, viv)]
    ow_in = fetch(ow_hbm, ow)

    barrier = pltpu.get_barrier_semaphore()
    peers = [near(r, 0) for r in (1, 2, 3)] + [near(0, s) for s in (1, 2, 3)]
    peers += [{"kv": kv, "tp": tp_at(*o)} for o in ORDER[:-1]]
    for peer in peers:
        pl.semaphore_signal(barrier, inc=1, device_id=peer, device_id_type=MESH)

    started = []

    def remote(src, dst, ssem, rsem, dev):
        return pltpu.make_async_remote_copy(
            src_ref=src, dst_ref=dst, send_sem=ssem, recv_sem=rsem, device_id=dev, device_id_type=MESH
        )

    def go(copy):
        copy.start()
        started.append(copy)

    half = NB // 2

    def a_copy(slot, part, r):
        rows = pl.ds(part * half, half)
        i = (slot // 2) * 2 + part
        return remote(kvb.at[rows], full[slot].at[rows], a_send.at[i], a_recv.at[i], near(r, 0))

    def af_copy(slot, part, r):
        rows = pl.ds(part * half, half)
        return remote(full[slot].at[rows], full2.at[rows], af_send.at[part], af_recv.at[part], near(r, 0))

    gain = gain_ref[...].astype(F32).reshape(1, D)
    for copy in w_in:
        copy.wait()
    for k in range(0, 256, 64):
        w1[k:k + 64, :] = (wst[k:k + 64, :].astype(F32) * gain).astype(BF)
    low = lanes((QB, 128)) < HD
    low64 = lanes((64, 128)) < HD
    front = (lanes((QB, 128)) % 64) < 32

    def turn(v, rows):
        other = jnp.where(front, pltpu.roll(v, 96, 1), pltpu.roll(v, 32, 1))
        return v * cos_s[rows, :] + other * sin_s[rows, :]

    embed = jnp.concatenate([ke_ref[...], ve_ref[...]], axis=1).astype(F32)
    embed = jnp.concatenate([embed] * (QB // CMP), axis=0)
    for t in range(tiles):
        t_in[t].wait()
        if t == 0:
            for copy in a_in:
                copy.wait()
        rows = pl.ds(t * TILE, TILE)
        x = tok[rows, :]
        proj = lax.dot_general(x, w1[...], NT, preferred_element_type=F32)
        xf = x.astype(F32)
        inv = lax.rsqrt(jnp.mean(xf * xf, axis=1, keepdims=True) + EPS)
        inv = jnp.broadcast_to(inv, (TILE, 128))
        inv_s[rows, :] = inv
        for j in range(TILE // QB):
            part = pl.ds(t * TILE + j * QB, QB)
            for u in (0, 1):
                g = t * (TILE // 64) + 2 * j + u
                cc, cs = ccv[g:g + 1, :], csv[g:g + 1, :]
                cos_s[pl.ds(g * 64, 64), :] = cc * fc_ref[...] - cs * fs_ref[...]
                sin_s[pl.ds(g * 64, 64), :] = (cs * fc_ref[...] + cc * fs_ref[...]) * sg_ref[...]
            scale = inv[j * QB:(j + 1) * QB]
            sel = proj[j * QB:(j + 1) * QB, 0:128] * scale
            sel = jnp.where(low, turn(sel, part), sel)
            vt = sel.T[64:128]
            b = t * (TILE // SEL) + 2 * j
            kvb[b] = jnp.where(low64, sel[0:64], pltpu.roll(vt, 64, 1)).astype(BF)
            kvb[b + 1] = jnp.where(low64, sel[64:128], vt).astype(BF)
            val = (proj[j * QB:(j + 1) * QB, 128:256] * scale).astype(BF).astype(F32) + embed
            raw[part, :] = val.astype(BF).astype(F32)
        if t % 2 == 1:
            if t == 1:
                pl.semaphore_wait(barrier, len(peers))
            for slot, r in ((3, 1), (1, 3)):
                go(a_copy(slot, t // 2, r))

    for copy in i_in:
        copy.wait()
    keys, values = [], []
    for r in range(0, CMP, 2):
        one = raw[pl.ds(r, 64, stride=CMP), :]
        two = raw[pl.ds(r + 1, 64, stride=CMP), :]
        keys.append(jnp.where(low64, one, pltpu.roll(two, 64, 1)).astype(BF))
        values.append(jnp.where(low64, pltpu.roll(one, 64, 1), two).astype(BF))
    parts = []
    for rows, inner, outer in ((keys, kiv, ko_ref), (values, viv, vo_ref)):
        flat = jnp.concatenate(rows, axis=1)
        hidden = gelu(lax.dot_general(flat, inner[...], NT, preferred_element_type=F32)).astype(BF)
        parts.append(jnp.dot(hidden, outer[...], preferred_element_type=F32))
    both = jnp.concatenate(parts, axis=1)
    own[...] = jnp.where(low64, both, jnp.concatenate([both, both], axis=0).T[64:128]).astype(BF)
    sums[0, 0] = own[...]

    def s_copy(r):
        return remote(own, sums.at[0, 4 - r], s_send.at[r - 1], s_recv.at[3 - r], near(r, 0))

    def s_bundle(s):
        return remote(sums.at[0], sums.at[4 - s], s_send.at[2 + s], s_recv.at[6 - s], near(0, s))

    for r in (1, 2, 3):
        go(s_copy(r))

    def dest_of(c):
        dest = 0
        for k in range(8):
            dest = dest + jnp.where(c == k, tp_at(*ORDER[k]), 0)
        return dest

    def select(r, g):
        span = at(r, 0)
        dests = [at(0, s) for s in range(4)]

        def body(c, _):
            q0 = dest_of(c) * 2
            for k in (0, 1):
                for s in range(4):
                    blk = tab[span, dests[s] * 16 + q0 + k] & (NB - 1)
                    val = full[r][blk]
                    if s == 0:
                        inb[r, 0, 2 * c + k] = val
                    else:
                        outb[r, s - 1, 2 * c + k] = val
            return 0

        lax.fori_loop(4 * g, 4 * g + 4, body, 0)

    def f_copy(r, g, k):
        part = pl.ds(8 * g + 4 * k, 4)
        return remote(
            outb.at[r, 1, part], fwd.at[r, g, k], f_send.at[r, 2 * g + k], f_recv.at[r, 2 * g + k],
            near(0, 1 + 2 * k),
        )

    def b_copy(r, g, k):
        part = pl.ds(8 * g, 8)
        return remote(
            outb.at[r, 2 * k, part], inb.at[r, 3 - 2 * k, part], b_send.at[r, g, k], b_recv.at[r, g, k],
            near(0, 1 + 2 * k),
        )

    def bf_copy(r, g, k):
        part = pl.ds(8 * g + 4 * k, 4)
        return remote(
            fwd.at[r, g, k], inb.at[r, 2, part], b_send.at[r, g, 2 + k], b_recv.at[r, g, 2 + k],
            near(0, 1 + 2 * k),
        )

    def b_start(r, g):
        for k in (0, 1):
            go(f_copy(r, g, k))
        for k in (0, 1):
            go(b_copy(r, g, k))

    def b_forward(r, g):
        for k in (0, 1):
            f_copy(r, g, k).wait_recv()
            go(bf_copy(r, g, k))

    def b_wait(r, g):
        for k in (0, 1):
            b_copy(r, g, k).wait_recv()
            bf_copy(r, g, k).wait_recv()

    select(0, 0)
    select(0, 1)

    for copy in q_in:
        copy.wait()
    w2[0:128, :] = (wqv[...].T.astype(F32) * gain).astype(BF)
    row = rows_of((128, 16))
    col = lanes((128, 16))
    e0 = jnp.where((row < 2) & (col == 2 * tp + row), 1.0, 0.0).astype(BF)
    e1 = jnp.where((row >= 2) & (row < 4) & (col == 2 * tp + row - 2), 1.0, 0.0).astype(BF)
    picked = jnp.dot(e0, bwv[0], preferred_element_type=F32) + jnp.dot(e1, bwv[1], preferred_element_type=F32)
    w2[128:256, :] = (picked * gain).astype(BF)
    zero = jnp.zeros((64, 256), BF)

    def queries(t):
        rows = pl.ds(t * TILE, TILE)
        proj = lax.dot_general(tok[rows, :], w2[...], NT, preferred_element_type=F32)
        for j in range(TILE // QB):
            part = pl.ds(t * TILE + j * QB, QB)
            q = t * (TILE // QB) + j
            scale = inv_s[part, :]
            v = proj[j * QB:(j + 1) * QB, 0:128] * scale
            for ref, val in ((qc, v), (qs, turn(v, part))):
                val = (val.T.astype(BF).astype(F32) * 0.125).astype(BF)
                ref[q, 0:64, 0:128] = val[0:64]
                ref[q, 0:64, 128:256] = val[64:128]
                ref[q, 64:128, :] = zero
            g = proj[j * QB:(j + 1) * QB, 128:256] * scale
            gt[q] = 1.0 / (1.0 + jnp.exp(-g.T[0:8]))

    queries(0)
    queries(1)
    for r in (1, 2, 3):
        s_copy(r).wait_recv()
    for s in (1, 2, 3):
        go(s_bundle(s))
    b_start(0, 0)
    b_start(0, 1)
    queries(2)
    queries(3)

    def values_of(blocks):
        pairs = [
            jnp.concatenate([blocks[k][:, HD:], blocks[k + 1][:, HD:]], axis=1) for k in range(0, len(blocks), 2)
        ]
        vt = jnp.concatenate(pairs, axis=1)
        return jnp.concatenate([vt, jnp.ones((16, vt.shape[1]), BF)], axis=0)

    def top(s):
        return jnp.max(s, axis=0, keepdims=True)

    def own_block(c, _):
        q0 = dest_of(c) * 2
        for k in (0, 1):
            q, i = q0 + k, 2 * c + k
            blocks = [kvb[2 * q], kvb[2 * q + 1]]
            s = jnp.dot(jnp.concatenate(blocks, axis=0), qs[q], preferred_element_type=F32)
            s = jnp.where(rows_of(s.shape) <= (lanes(s.shape) & (QB - 1)), s, NEG)
            m = top(s)
            mrow[i] = m
            acc[i] = jnp.dot(values_of(blocks), jnp.exp(s - m).astype(BF), preferred_element_type=F32)
        return 0

    def far_step(q, i, r):
        blocks = [inb[r, s, i] for s in range(4)]
        sc = jnp.dot(jnp.concatenate(blocks, axis=0), qs[q], preferred_element_type=F32)
        m = old = mrow[i]
        bias = []
        for s in range(4):
            used = lax.shift_right_logical(tab[at(r, s), kv * 16 + q], 6)
            bias.append((used.astype(F32) - 1.0) * 1e30)
            m = jnp.maximum(m, top(sc[64 * s:64 * s + 64]) + bias[s])
        p = [jnp.exp(sc[64 * s:64 * s + 64] - (m - bias[s])).astype(BF) for s in range(4)]
        add = jnp.dot(values_of(blocks), jnp.concatenate(p, axis=0), preferred_element_type=F32)
        return m, acc[i] * jnp.exp(old - m) + add

    def far(r, g):
        def body(c, _):
            q0 = dest_of(c) * 2
            new = [far_step(q0 + k, 2 * c + k, r) for k in (0, 1)]
            for k in (0, 1):
                mrow[2 * c + k] = new[k][0]
                acc[2 * c + k] = new[k][1]
            return 0

        lax.fori_loop(4 * g, 4 * g + 4, body, 0)

    def compressed(c, _):
        q0 = dest_of(c) * 2
        for k in (0, 1):
            q, i = q0 + k, 2 * c + k
            scs, ms = [], []
            m = jnp.full((1, 256), FLOOR, F32)
            for s in range(4):
                sc = jnp.dot(sums[s].reshape(256, 128), qc[q], preferred_element_type=F32)
                for r in range(4):
                    one = sc[64 * r:64 * r + 64]
                    bias = jnp.where(at(r, s) < kv, 0.0, NEG)
                    if r == 0 and s == 0:
                        end = (rows_of(one.shape) + 1) * CMP - 1
                        one = jnp.where(end <= q * QB + (lanes(one.shape) & (QB - 1)), one, NEG)
                        bias = 0.0
                    scs.append(one)
                    ms.append(bias)
                    m = jnp.maximum(m, top(one) + bias)
            total = jnp.zeros((80, 256), F32)
            for s in range(4):
                p = [jnp.exp(scs[4 * s + r] - (m - ms[4 * s + r])).astype(BF) for r in range(4)]
                total += jnp.dot(
                    vtc[:, 256 * s:256 * s + 256], jnp.concatenate(p, axis=0), preferred_element_type=F32
                )
            den = total[64:65]
            ocmp[i] = jnp.where(den > 0, total[0:64] / jnp.maximum(den, 1e-30), 0.0)
        return 0

    def finish(c):
        q0 = tp_at(*ORDER[c]) * 2
        for k in (0, 1):
            q, i = q0 + k, 2 * c + k
            _, a = far_step(q, i, 2)
            o = a[0:64] / a[64:65]
            oc = ocmp[i]
            g = gt[q]
            heads = [
                g[h:h + 1] * oc[:, 128 * h:128 * h + 128] + g[2 + h:3 + h] * o[:, 128 * h:128 * h + 128]
                for h in (0, 1)
            ]
            mix[c, k * QB:(k + 1) * QB, :] = jnp.concatenate(heads, axis=0).T.astype(BF)

    def t_copy(c, slot):
        return remote(mix.at[c], hr.at[slot], t_send.at[c], t_recv.at[c], {"kv": kv, "tp": tp_at(*ORDER[c])})

    lax.fori_loop(0, 8, own_block, 0)
    for s in (1, 2, 3):
        s_bundle(s).wait_recv()
    for s in range(4):
        vtc[:, 256 * s:256 * s + 256] = values_of([sums[s, r] for r in range(4)])
    lax.fori_loop(0, 2, compressed, 0)
    a_copy(3, 0, 1).wait_recv()
    go(af_copy(3, 0, 1))
    lax.fori_loop(2, 4, compressed, 0)
    b_forward(0, 0)
    a_copy(1, 1, 1).wait_recv()
    go(af_copy(1, 1, 3))
    a_copy(3, 1, 1).wait_recv()
    select(3, 0)
    b_start(3, 0)
    a_copy(1, 0, 1).wait_recv()
    select(1, 0)
    b_start(1, 0)
    b_forward(0, 1)
    select(3, 1)
    select(1, 1)
    lax.fori_loop(4, 6, compressed, 0)
    af_copy(3, 0, 1).wait_recv()
    af_copy(1, 1, 1).wait_recv()
    select(2, 0)
    b_start(2, 0)
    b_start(3, 1)
    b_start(1, 1)
    select(2, 1)
    b_start(2, 1)
    lax.fori_loop(6, 8, compressed, 0)
    b_forward(3, 0)
    b_forward(1, 0)
    b_wait(0, 0)
    far(0, 0)
    b_forward(2, 0)
    b_wait(0, 1)
    far(0, 1)
    b_wait(3, 0)
    far(3, 0)
    b_forward(3, 1)
    b_wait(1, 0)
    far(1, 0)
    b_forward(1, 1)
    b_wait(2, 0)
    for c in range(4):
        finish(c)
        go(t_copy(c, tp))
    b_forward(2, 1)
    b_wait(3, 1)
    far(3, 1)
    b_wait(1, 1)
    far(1, 1)
    b_wait(2, 1)
    for c in range(4, 7):
        finish(c)
        go(t_copy(c, tp))
    finish(7)
    hr[tp] = mix[7]

    ow_in.wait()
    for c in range(7):
        dy, dc = ORDER[c]
        t_copy(c, tp_at((4 - dy) % 4, dc)).wait_recv()
    x = jnp.concatenate([hr[t] for t in range(8)], axis=1)
    outs = []
    for n in range(4):
        cols = pl.ds(n * 512, 512)
        res[:, cols] = jnp.dot(x, ow[:, cols], preferred_element_type=F32).astype(BF)
        copy = pltpu.make_async_copy(res.at[:, cols], out_hbm.at[:, cols], o_sem.at[n])
        copy.start()
        outs.append(copy)
    for copy in started:
        copy.wait_send()
    for copy in outs:
        copy.wait()


def pick_table(chosen):
    picks = chosen[0].T
    block = jnp.arange(256, dtype=jnp.int32)[None, :]
    code = (picks & (NB - 1)) + jnp.where(picks < 2 * block, 64, 0)
    match = (picks >> 5)[None] == jnp.arange(16, dtype=jnp.int32)[:, None, None]
    return jnp.sum(jnp.where(match, code[None], 0), axis=1)


def per_device(
    tokens, norm_gain, query_weight, cmp_key_weight, cmp_value_weight, sel_key_weight, sel_value_weight,
    branch_weight, key_embed, key_inner, key_outer, value_embed, value_inner, value_outer, out_weight, chosen,
):
    cc, cs, fc, fs, sg = angle_tables()
    vm = pl.BlockSpec(memory_space=pltpu.VMEM)
    hbm = pl.BlockSpec(memory_space=pl.ANY)
    dma = pltpu.SemaphoreType.DMA
    v = pltpu.VMEM
    return pl.pallas_call(
        kernel,
        in_specs=[pl.BlockSpec(memory_space=pltpu.SMEM)] + [vm] * 8 + [hbm] * 12,
        out_specs=hbm,
        out_shape=jax.ShapeDtypeStruct((256, D), BF),
        scratch_shapes=[
            v((TOK, D), BF), v((256, D), BF), v((256, D), BF), v((D, 128), BF), v((2, 16, D), BF), v((256, D), BF),
            v((64, D), BF), v((64, D), BF), v((32, 128), F32), v((32, 128), F32), v((1024, D), BF),
            v((TOK, 128), F32), v((TOK, 128), F32), v((TOK, 128), F32), v((TOK, 128), F32),
            v((NQ, 128, 256), BF), v((NQ, 128, 256), BF), v((NQ, 8, 128), F32),
            v((NB, SEL, 128), BF), v((NB, SEL, 128), BF), v((NB, SEL, 128), BF), v((NB, SEL, 128), BF),
            v((4, 4, NQ, SEL, 128), BF), v((4, 3, NQ, SEL, 128), BF), v((4, 2, 2, 4, SEL, 128), BF),
            v((64, 128), BF), v((4, 4, 64, 128), BF), v((80, 1024), BF),
            v((NQ, 80, 256), F32), v((NQ, 1, 256), F32), v((NQ, 64, 256), F32),
            v((8, 256, 128), BF), v((8, 256, 128), BF), v((256, D), BF),
            dma((16,)), dma((4,)), dma((4,)), dma((2,)), dma((2,)), dma((6,)), dma((6,)),
            dma((4, 2, 4)), dma((4, 2, 4)), dma((4, 4)), dma((4, 4)), dma((8,)), dma((8,)), dma((4,)),
        ],
        compiler_params=pltpu.CompilerParams(collective_id=0, has_side_effects=True, vmem_limit_bytes=67043328),
        name="layer",
    )(
        pick_table(chosen), norm_gain, key_embed[0], key_outer[0], value_embed[0], value_outer[0], fc, fs, sg,
        tokens, query_weight, cmp_key_weight.T, cmp_value_weight.T, sel_key_weight.T, sel_value_weight.T,
        branch_weight.transpose(0, 2, 1), key_inner[0].T, value_inner[0].T, cc, cs, out_weight,
    )


def solution(mesh):
    placed = (
        P("kv", None), P(), P(None, "tp"), P(None, "tp"), P(None, "tp"), P(None, "tp"), P(None, "tp"), P(),
        P("tp", None, None), P("tp", None, None), P("tp", None, None), P("tp", None, None),
        P("tp", None, None), P("tp", None, None), P(), P("tp", None, None),
    )
    return jax.shard_map(
        per_device, mesh=mesh, in_specs=placed, out_specs=P(("kv", "tp"), None), check_vma=False
    )
```

```python
import jax
import jax.numpy as jnp
import numpy as np
from jax import lax
from jax.experimental import pallas as pl
from jax.experimental.pallas import tpu as pltpu
from jax.sharding import PartitionSpec as P

D = 2048
HD = 64
CMP = 32
SEL = 64
QB = 128
TOK = 2048
NQ = TOK // QB
NB = TOK // SEL
EPS = 1e-06
NEG = -1e30
FLOOR = -1e20
TILE = 512
MESH = pl.DeviceIdType.MESH
NT = (((1,), (1,)), ((), ()))
BF = jnp.bfloat16
F32 = jnp.float32
ORDER = ((2, 0), (2, 1), (1, 0), (3, 0), (1, 1), (3, 1), (0, 1), (0, 0))


def angle_tables():
    lane = np.arange(128)
    freq = 10000.0 ** (-(lane % 32) / 32.0)
    sign = np.where(lane % 64 < 32, -1.0, 1.0)
    coarse = np.arange(512)[:, None] * 64.0 * freq
    fine = np.arange(64)[:, None] * freq
    as32 = lambda t: jnp.asarray(np.asarray(t, np.float32))
    return as32(np.cos(coarse)), as32(np.sin(coarse)), as32(np.cos(fine)), as32(np.sin(fine)), as32(sign[None])


def lanes(shape):
    return lax.broadcasted_iota(jnp.int32, shape, 1)


def rows_of(shape):
    return lax.broadcasted_iota(jnp.int32, shape, 0)


def gelu(x):
    return 0.5 * x * (1.0 + jnp.tanh(0.7978845608028654 * (x + 0.044715 * (x * x * x))))


def kernel(
    tab, gain_ref, ke_ref, ko_ref, ve_ref, vo_ref, fc_ref, fs_ref, sg_ref,
    tok_hbm, wq_hbm, wck_hbm, wcv_hbm, wsk_hbm, wsv_hbm, bw_hbm, ki_hbm, vi_hbm, cc_hbm, cs_hbm, ow_hbm,
    out_hbm,
    tok, wst, w1, wqv, bwv, w2, kiv, viv, ccv, csv, ow, inv_s, cos_s, sin_s, raw, qs, qc, gt,
    kvb, full1, full2, full3, inb, outb, fwd, own, sums, vtc, acc, mrow, ocmp, mix, hr, res,
    l_sem, a_send, a_recv, af_send, af_recv, s_send, s_recv, b_send, b_recv, f_send, f_recv, t_send, t_recv, o_sem,
):
    full = (kvb, full1, full2, full3)
    tp = lax.axis_index("tp")
    kv = lax.axis_index("kv")
    core = lax.rem(tp, 2)
    yy = tp // 2
    zz = kv // 4
    xx = lax.rem(kv, 4)
    sa = 4 - 3 * core
    sb = 1 + 3 * core
    aa = zz * (1 - core) + xx * core
    bb = xx * (1 - core) + zz * core

    def at(r, s):
        return lax.rem(aa + r, 4) * sa + lax.rem(bb + s, 4) * sb

    def tp_at(dy, dc):
        return 2 * lax.rem(yy + dy, 4) + (core + dc - 2 * core * dc)

    def near(r, s):
        return {"kv": at(r, s), "tp": tp}

    local = []

    def fetch(src, dst):
        copy = pltpu.make_async_copy(src, dst, l_sem.at[len(local)])
        copy.start()
        local.append(copy)
        return copy

    w_in = [fetch(h, wst.at[pl.ds(64 * k, 64)]) for k, h in enumerate((wsk_hbm, wsv_hbm, wck_hbm, wcv_hbm))]
    tiles = TOK // TILE

    def tok_in(t):
        return fetch(tok_hbm.at[pl.ds(t * TILE, TILE)], tok.at[pl.ds(t * TILE, TILE)])

    t_in = [tok_in(0)]
    base = pl.ds(pl.multiple_of(kv * 32, 32), 32)
    a_in = [fetch(cc_hbm.at[base], ccv), fetch(cs_hbm.at[base], csv)]
    t_in += [tok_in(1), tok_in(2), tok_in(3)]
    q_in = [fetch(wq_hbm, wqv), fetch(bw_hbm, bwv)]
    i_in = [fetch(ki_hbm, kiv), fetch(vi_hbm, viv)]
    ow_in = fetch(ow_hbm, ow)

    barrier = pltpu.get_barrier_semaphore()
    peers = [near(r, 0) for r in (1, 2, 3)] + [near(0, s) for s in (1, 2, 3)]
    peers += [{"kv": kv, "tp": tp_at(*o)} for o in ORDER[:-1]]
    for peer in peers:
        pl.semaphore_signal(barrier, inc=1, device_id=peer, device_id_type=MESH)

    started = []

    def remote(src, dst, ssem, rsem, dev):
        return pltpu.make_async_remote_copy(
            src_ref=src, dst_ref=dst, send_sem=ssem, recv_sem=rsem, device_id=dev, device_id_type=MESH
        )

    def go(copy):
        copy.start()
        started.append(copy)

    half = NB // 2

    def a_copy(slot, part, r):
        rows = pl.ds(part * half, half)
        i = (slot // 2) * 2 + part
        return remote(kvb.at[rows], full[slot].at[rows], a_send.at[i], a_recv.at[i], near(r, 0))

    def af_copy(slot, part, r):
        rows = pl.ds(part * half, half)
        return remote(full[slot].at[rows], full2.at[rows], af_send.at[part], af_recv.at[part], near(r, 0))

    gain = gain_ref[...].astype(F32).reshape(1, D)
    for copy in w_in:
        copy.wait()
    for k in range(0, 256, 64):
        w1[k:k + 64, :] = (wst[k:k + 64, :].astype(F32) * gain).astype(BF)
    low = lanes((QB, 128)) < HD
    low64 = lanes((64, 128)) < HD
    front = (lanes((QB, 128)) % 64) < 32

    def turn(v, rows):
        other = jnp.where(front, pltpu.roll(v, 96, 1), pltpu.roll(v, 32, 1))
        return v * cos_s[rows, :] + other * sin_s[rows, :]

    embed = jnp.concatenate([ke_ref[...], ve_ref[...]], axis=1).astype(F32)
    embed = jnp.concatenate([embed] * (QB // CMP), axis=0)
    for t in range(tiles):
        t_in[t].wait()
        if t == 0:
            for copy in a_in:
                copy.wait()
        rows = pl.ds(t * TILE, TILE)
        x = tok[rows, :]
        proj = lax.dot_general(x, w1[...], NT, preferred_element_type=F32)
        xf = x.astype(F32)
        inv = lax.rsqrt(jnp.mean(xf * xf, axis=1, keepdims=True) + EPS)
        inv = jnp.broadcast_to(inv, (TILE, 128))
        inv_s[rows, :] = inv
        for j in range(TILE // QB):
            part = pl.ds(t * TILE + j * QB, QB)
            for u in (0, 1):
                g = t * (TILE // 64) + 2 * j + u
                cc, cs = ccv[g:g + 1, :], csv[g:g + 1, :]
                cos_s[pl.ds(g * 64, 64), :] = cc * fc_ref[...] - cs * fs_ref[...]
                sin_s[pl.ds(g * 64, 64), :] = (cs * fc_ref[...] + cc * fs_ref[...]) * sg_ref[...]
            scale = inv[j * QB:(j + 1) * QB]
            sel = proj[j * QB:(j + 1) * QB, 0:128] * scale
            sel = jnp.where(low, turn(sel, part), sel)
            vt = sel.T[64:128]
            b = t * (TILE // SEL) + 2 * j
            kvb[b] = jnp.where(low64, sel[0:64], pltpu.roll(vt, 64, 1)).astype(BF)
            kvb[b + 1] = jnp.where(low64, sel[64:128], vt).astype(BF)
            val = (proj[j * QB:(j + 1) * QB, 128:256] * scale).astype(BF).astype(F32) + embed
            raw[part, :] = val.astype(BF).astype(F32)
        if t % 2 == 1:
            if t == 1:
                pl.semaphore_wait(barrier, len(peers))
            for slot, r in ((3, 1), (1, 3)):
                go(a_copy(slot, t // 2, r))

    for copy in i_in:
        copy.wait()
    keys, values = [], []
    for r in range(0, CMP, 2):
        one = raw[pl.ds(r, 64, stride=CMP), :]
        two = raw[pl.ds(r + 1, 64, stride=CMP), :]
        keys.append(jnp.where(low64, one, pltpu.roll(two, 64, 1)).astype(BF))
        values.append(jnp.where(low64, pltpu.roll(one, 64, 1), two).astype(BF))
    parts = []
    for rows, inner, outer in ((keys, kiv, ko_ref), (values, viv, vo_ref)):
        flat = jnp.concatenate(rows, axis=1)
        hidden = gelu(lax.dot_general(flat, inner[...], NT, preferred_element_type=F32)).astype(BF)
        parts.append(jnp.dot(hidden, outer[...], preferred_element_type=F32))
    both = jnp.concatenate(parts, axis=1)
    own[...] = jnp.where(low64, both, jnp.concatenate([both, both], axis=0).T[64:128]).astype(BF)
    sums[0, 0] = own[...]

    def s_copy(r):
        return remote(own, sums.at[0, 4 - r], s_send.at[r - 1], s_recv.at[3 - r], near(r, 0))

    def s_bundle(s):
        return remote(sums.at[0], sums.at[4 - s], s_send.at[2 + s], s_recv.at[6 - s], near(0, s))

    for r in (1, 2, 3):
        go(s_copy(r))

    def dest_of(c):
        dest = 0
        for k in range(8):
            dest = dest + jnp.where(c == k, tp_at(*ORDER[k]), 0)
        return dest

    def select(r, g):
        span = at(r, 0)
        dests = [at(0, s) for s in range(4)]

        def body(c, _):
            q0 = dest_of(c) * 2
            for k in (0, 1):
                for s in range(4):
                    blk = tab[span, dests[s] * 16 + q0 + k] & (NB - 1)
                    val = full[r][blk]
                    if s == 0:
                        inb[r, 0, 2 * c + k] = val
                    else:
                        outb[r, s - 1, 2 * c + k] = val
            return 0

        lax.fori_loop(4 * g, 4 * g + 4, body, 0)

    def f_copy(r, g, k):
        part = pl.ds(8 * g + 4 * k, 4)
        return remote(
            outb.at[r, 1, part], fwd.at[r, g, k], f_send.at[r, 2 * g + k], f_recv.at[r, 2 * g + k],
            near(0, 1 + 2 * k),
        )

    def b_copy(r, g, k):
        part = pl.ds(8 * g, 8)
        return remote(
            outb.at[r, 2 * k, part], inb.at[r, 3 - 2 * k, part], b_send.at[r, g, k], b_recv.at[r, g, k],
            near(0, 1 + 2 * k),
        )

    def bf_copy(r, g, k):
        part = pl.ds(8 * g + 4 * k, 4)
        return remote(
            fwd.at[r, g, k], inb.at[r, 2, part], b_send.at[r, g, 2 + k], b_recv.at[r, g, 2 + k],
            near(0, 1 + 2 * k),
        )

    def f_start(r, g):
        for k in (0, 1):
            go(f_copy(r, g, k))

    def d_start(r, g):
        for k in (0, 1):
            go(b_copy(r, g, k))

    def b_start(r, g):
        f_start(r, g)
        d_start(r, g)

    def b_forward(r, g):
        for k in (0, 1):
            f_copy(r, g, k).wait_recv()
            go(bf_copy(r, g, k))

    def b_wait(r, g):
        for k in (0, 1):
            b_copy(r, g, k).wait_recv()
            bf_copy(r, g, k).wait_recv()

    select(0, 0)
    select(0, 1)

    for copy in q_in:
        copy.wait()
    w2[0:128, :] = (wqv[...].T.astype(F32) * gain).astype(BF)
    row = rows_of((128, 16))
    col = lanes((128, 16))
    e0 = jnp.where((row < 2) & (col == 2 * tp + row), 1.0, 0.0).astype(BF)
    e1 = jnp.where((row >= 2) & (row < 4) & (col == 2 * tp + row - 2), 1.0, 0.0).astype(BF)
    picked = jnp.dot(e0, bwv[0], preferred_element_type=F32) + jnp.dot(e1, bwv[1], preferred_element_type=F32)
    w2[128:256, :] = (picked * gain).astype(BF)
    zero = jnp.zeros((64, 256), BF)

    def queries(t):
        rows = pl.ds(t * TILE, TILE)
        proj = lax.dot_general(tok[rows, :], w2[...], NT, preferred_element_type=F32)
        for j in range(TILE // QB):
            part = pl.ds(t * TILE + j * QB, QB)
            q = t * (TILE // QB) + j
            scale = inv_s[part, :]
            v = proj[j * QB:(j + 1) * QB, 0:128] * scale
            for ref, val in ((qc, v), (qs, turn(v, part))):
                val = (val.T.astype(BF).astype(F32) * 0.125).astype(BF)
                ref[q, 0:64, 0:128] = val[0:64]
                ref[q, 0:64, 128:256] = val[64:128]
                ref[q, 64:128, :] = zero
            g = proj[j * QB:(j + 1) * QB, 128:256] * scale
            gt[q] = 1.0 / (1.0 + jnp.exp(-g.T[0:8]))

    queries(0)
    queries(1)
    for r in (1, 2, 3):
        s_copy(r).wait_recv()
    for s in (1, 2, 3):
        go(s_bundle(s))
    b_start(0, 0)
    b_start(0, 1)
    a_copy(3, 0, 1).wait_recv()
    go(af_copy(3, 0, 1))
    queries(2)
    queries(3)

    def values_of(blocks):
        pairs = [
            jnp.concatenate([blocks[k][:, HD:], blocks[k + 1][:, HD:]], axis=1) for k in range(0, len(blocks), 2)
        ]
        vt = jnp.concatenate(pairs, axis=1)
        return jnp.concatenate([vt, jnp.ones((16, vt.shape[1]), BF)], axis=0)

    def top(s):
        return jnp.max(s, axis=0, keepdims=True)

    def own_group(g):
        ids = [(tp_at(*ORDER[c]) * 2 + k, 2 * c + k) for c in range(4 * g, 4 * g + 4) for k in (0, 1)]
        blocks = [[kvb[2 * q], kvb[2 * q + 1]] for q, _ in ids]
        scs = [
            jnp.dot(jnp.concatenate(blk, axis=0), qs[q], preferred_element_type=F32)
            for blk, (q, _) in zip(blocks, ids)
        ]
        ps = []
        for sc, (_, i) in zip(scs, ids):
            sc = jnp.where(rows_of(sc.shape) <= (lanes(sc.shape) & (QB - 1)), sc, NEG)
            m = top(sc)
            mrow[i] = m
            ps.append(jnp.exp(sc - m).astype(BF))
        for p, blk, (_, i) in zip(ps, blocks, ids):
            acc[i] = jnp.dot(values_of(blk), p, preferred_element_type=F32)

    def far_steps(ids, r):
        blocks = [[inb[r, s, i] for s in range(4)] for _, i in ids]
        scs = [
            jnp.dot(jnp.concatenate(blk, axis=0), qs[q], preferred_element_type=F32)
            for blk, (q, _) in zip(blocks, ids)
        ]
        ms, ps, scale = [], [], []
        for sc, (q, i) in zip(scs, ids):
            m = old = mrow[i]
            bias = []
            for s in range(4):
                used = lax.shift_right_logical(tab[at(r, s), kv * 16 + q], 6)
                bias.append((used.astype(F32) - 1.0) * 1e30)
                m = jnp.maximum(m, top(sc[64 * s:64 * s + 64]) + bias[s])
            p = [jnp.exp(sc[64 * s:64 * s + 64] - (m - bias[s])).astype(BF) for s in range(4)]
            ms.append(m)
            ps.append(jnp.concatenate(p, axis=0))
            scale.append(jnp.exp(old - m))
        adds = [jnp.dot(values_of(blk), p, preferred_element_type=F32) for blk, p in zip(blocks, ps)]
        return ms, [acc[i] * sc + add for (_, i), sc, add in zip(ids, scale, adds)]

    def ids_of(c0, n):
        return [(tp_at(*ORDER[c]) * 2 + k, 2 * c + k) for c in range(c0, c0 + n) for k in (0, 1)]

    def far_group(g):
        ids = ids_of(4 * g, 4)

        def body(n, _):
            ms, accs = far_steps(ids, n + n // 2)
            for (_, i), m, a in zip(ids, ms, accs):
                mrow[i] = m
                acc[i] = a
            return 0

        lax.fori_loop(0, 3, body, 0)

    def compressed(c, _):
        q0 = dest_of(c) * 2
        for k in (0, 1):
            q, i = q0 + k, 2 * c + k
            scs, ms = [], []
            m = jnp.full((1, 256), FLOOR, F32)
            for s in range(4):
                sc = jnp.dot(sums[s].reshape(256, 128), qc[q], preferred_element_type=F32)
                for r in range(4):
                    one = sc[64 * r:64 * r + 64]
                    bias = jnp.where(at(r, s) < kv, 0.0, NEG)
                    if r == 0 and s == 0:
                        end = (rows_of(one.shape) + 1) * CMP - 1
                        one = jnp.where(end <= q * QB + (lanes(one.shape) & (QB - 1)), one, NEG)
                        bias = 0.0
                    scs.append(one)
                    ms.append(bias)
                    m = jnp.maximum(m, top(one) + bias)
            total = jnp.zeros((80, 256), F32)
            for s in range(4):
                p = [jnp.exp(scs[4 * s + r] - (m - ms[4 * s + r])).astype(BF) for r in range(4)]
                total += jnp.dot(
                    vtc[:, 256 * s:256 * s + 256], jnp.concatenate(p, axis=0), preferred_element_type=F32
                )
            den = total[64:65]
            ocmp[i] = jnp.where(den > 0, total[0:64] / jnp.maximum(den, 1e-30), 0.0)
        return 0

    def finish(c0, n):
        ids = ids_of(c0, n)
        _, accs = far_steps(ids, 2)
        for (q, i), a in zip(ids, accs):
            o = a[0:64] / a[64:65]
            oc = ocmp[i]
            g = gt[q]
            heads = [
                g[h:h + 1] * oc[:, 128 * h:128 * h + 128] + g[2 + h:3 + h] * o[:, 128 * h:128 * h + 128]
                for h in (0, 1)
            ]
            mix[i // 2, (i % 2) * QB:(i % 2 + 1) * QB, :] = jnp.concatenate(heads, axis=0).T.astype(BF)

    def t_copy(c, slot):
        return remote(mix.at[c], hr.at[slot], t_send.at[c], t_recv.at[c], {"kv": kv, "tp": tp_at(*ORDER[c])})

    own_group(0)
    own_group(1)
    a_copy(1, 1, 1).wait_recv()
    go(af_copy(1, 1, 3))
    for s in (1, 2, 3):
        s_bundle(s).wait_recv()
    for s in range(4):
        vtc[:, 256 * s:256 * s + 256] = values_of([sums[s, r] for r in range(4)])
    lax.fori_loop(0, 2, compressed, 0)
    a_copy(3, 1, 1).wait_recv()
    a_copy(1, 0, 1).wait_recv()
    for r in (3, 1):
        select(r, 0)
        f_start(r, 0)
    for r in (3, 1):
        select(r, 1)
        f_start(r, 1)
    d_start(3, 0)
    d_start(1, 0)
    b_forward(0, 0)
    b_forward(0, 1)
    lax.fori_loop(2, 4, compressed, 0)
    af_copy(3, 0, 1).wait_recv()
    af_copy(1, 1, 1).wait_recv()
    for g in (0, 1):
        select(2, g)
        f_start(2, g)
    b_forward(3, 0)
    b_forward(1, 0)
    d_start(2, 0)
    lax.fori_loop(4, 6, compressed, 0)
    b_forward(2, 0)
    b_forward(3, 1)
    b_forward(1, 1)
    for r in (3, 1, 2):
        d_start(r, 1)
    lax.fori_loop(6, 8, compressed, 0)
    b_forward(2, 1)
    for g in (0, 1):
        for r in (0, 3, 1):
            b_wait(r, g)
        far_group(g)
        b_wait(2, g)
        for c in (4 * g, 4 * g + 2):
            finish(c, 2)
            for k in (c, c + 1):
                if k < 7:
                    go(t_copy(k, tp))
    hr[tp] = mix[7]

    ow_in.wait()
    for c in range(7):
        dy, dc = ORDER[c]
        t_copy(c, tp_at((4 - dy) % 4, dc)).wait_recv()
    x = jnp.concatenate([hr[t] for t in range(8)], axis=1)
    outs = []
    for n in range(4):
        cols = pl.ds(n * 512, 512)
        res[:, cols] = jnp.dot(x, ow[:, cols], preferred_element_type=F32).astype(BF)
        copy = pltpu.make_async_copy(res.at[:, cols], out_hbm.at[:, cols], o_sem.at[n])
        copy.start()
        outs.append(copy)
    for copy in started:
        copy.wait_send()
    for copy in outs:
        copy.wait()


def pick_table(chosen):
    picks = chosen[0].T
    block = jnp.arange(256, dtype=jnp.int32)[None, :]
    code = (picks & (NB - 1)) + jnp.where(picks < 2 * block, 64, 0)
    match = (picks >> 5)[None] == jnp.arange(16, dtype=jnp.int32)[:, None, None]
    return jnp.sum(jnp.where(match, code[None], 0), axis=1)


def per_device(
    tokens, norm_gain, query_weight, cmp_key_weight, cmp_value_weight, sel_key_weight, sel_value_weight,
    branch_weight, key_embed, key_inner, key_outer, value_embed, value_inner, value_outer, out_weight, chosen,
):
    cc, cs, fc, fs, sg = angle_tables()
    vm = pl.BlockSpec(memory_space=pltpu.VMEM)
    hbm = pl.BlockSpec(memory_space=pl.ANY)
    dma = pltpu.SemaphoreType.DMA
    v = pltpu.VMEM
    return pl.pallas_call(
        kernel,
        in_specs=[pl.BlockSpec(memory_space=pltpu.SMEM)] + [vm] * 8 + [hbm] * 12,
        out_specs=hbm,
        out_shape=jax.ShapeDtypeStruct((256, D), BF),
        scratch_shapes=[
            v((TOK, D), BF), v((256, D), BF), v((256, D), BF), v((D, 128), BF), v((2, 16, D), BF), v((256, D), BF),
            v((64, D), BF), v((64, D), BF), v((32, 128), F32), v((32, 128), F32), v((1024, D), BF),
            v((TOK, 128), F32), v((TOK, 128), F32), v((TOK, 128), F32), v((TOK, 128), F32),
            v((NQ, 128, 256), BF), v((NQ, 128, 256), BF), v((NQ, 8, 128), F32),
            v((NB, SEL, 128), BF), v((NB, SEL, 128), BF), v((NB, SEL, 128), BF), v((NB, SEL, 128), BF),
            v((4, 4, NQ, SEL, 128), BF), v((4, 3, NQ, SEL, 128), BF), v((4, 2, 2, 4, SEL, 128), BF),
            v((64, 128), BF), v((4, 4, 64, 128), BF), v((80, 1024), BF),
            v((NQ, 80, 256), F32), v((NQ, 1, 256), F32), v((NQ, 64, 256), F32),
            v((8, 256, 128), BF), v((8, 256, 128), BF), v((256, D), BF),
            dma((16,)), dma((4,)), dma((4,)), dma((2,)), dma((2,)), dma((6,)), dma((6,)),
            dma((4, 2, 4)), dma((4, 2, 4)), dma((4, 4)), dma((4, 4)), dma((8,)), dma((8,)), dma((4,)),
        ],
        compiler_params=pltpu.CompilerParams(collective_id=0, has_side_effects=True, vmem_limit_bytes=67043328),
        name="layer",
    )(
        pick_table(chosen), norm_gain, key_embed[0], key_outer[0], value_embed[0], value_outer[0], fc, fs, sg,
        tokens, query_weight, cmp_key_weight.T, cmp_value_weight.T, sel_key_weight.T, sel_value_weight.T,
        branch_weight.transpose(0, 2, 1), key_inner[0].T, value_inner[0].T, cc, cs, out_weight,
    )


def solution(mesh):
    placed = (
        P("kv", None), P(), P(None, "tp"), P(None, "tp"), P(None, "tp"), P(None, "tp"), P(None, "tp"), P(),
        P("tp", None, None), P("tp", None, None), P("tp", None, None), P("tp", None, None),
        P("tp", None, None), P("tp", None, None), P(), P("tp", None, None),
    )
    return jax.shard_map(
        per_device, mesh=mesh, in_specs=placed, out_specs=P(("kv", "tp"), None), check_vma=False
    )
```

```python
import jax
import jax.numpy as jnp
import numpy as np
from jax import lax
from jax.experimental import pallas as pl
from jax.experimental.pallas import tpu as pltpu
from jax.sharding import PartitionSpec as P

D = 2048
HD = 64
CMP = 32
SEL = 64
QB = 128
TOK = 2048
NQ = TOK // QB
NB = TOK // SEL
PITCH = 40
EPS = 1e-06
NEG = -1e30
FLOOR = -1e20
TILE = 512
MESH = pl.DeviceIdType.MESH
NT = (((1,), (1,)), ((), ()))
BF = jnp.bfloat16
F32 = jnp.float32
ORDER = ((2, 0), (2, 1), (1, 0), (3, 0), (1, 1), (3, 1), (0, 1), (0, 0))


def angle_tables():
    lane = np.arange(128)
    freq = 10000.0 ** (-(lane % 32) / 32.0)
    sign = np.where(lane % 64 < 32, -1.0, 1.0)
    coarse = np.arange(512)[:, None] * 64.0 * freq
    fine = np.arange(64)[:, None] * freq
    as32 = lambda t: jnp.asarray(np.asarray(t, np.float32))
    return as32(np.cos(coarse)), as32(np.sin(coarse)), as32(np.cos(fine)), as32(np.sin(fine)), as32(sign[None])


def lanes(shape):
    return lax.broadcasted_iota(jnp.int32, shape, 1)


def rows_of(shape):
    return lax.broadcasted_iota(jnp.int32, shape, 0)


def gelu(x):
    return 0.5 * x * (1.0 + jnp.tanh(0.7978845608028654 * (x + 0.044715 * (x * x * x))))


def kernel(
    picks_ref, gain_ref, ke_ref, ko_ref, ve_ref, vo_ref, fc_ref, fs_ref, sg_ref,
    tok_hbm, wq_hbm, wck_hbm, wcv_hbm, wsk_hbm, wsv_hbm, bw_hbm, ki_hbm, vi_hbm, cc_hbm, cs_hbm, ow_hbm,
    out_hbm,
    tab, tabv, tok, wst, w1, wqv, bwv, w2, kiv, viv, ccv, csv, ow, inv_s, cos_s, sin_s, raw, qs, qc, gt,
    kvb, full1, full2, full3, inb, outb, fwd, own, sums, vtc, acc, mrow, ocmp, mix, hr, res,
    l_sem, a_send, a_recv, af_send, af_recv, s_send, s_recv, b_send, b_recv, f_send, f_recv, t_send, t_recv, o_sem,
):
    full = (kvb, full1, full2, full3)
    tp = lax.axis_index("tp")
    kv = lax.axis_index("kv")
    core = lax.rem(tp, 2)
    yy = tp // 2
    zz = kv // 4
    xx = lax.rem(kv, 4)
    sa = 4 - 3 * core
    sb = 1 + 3 * core
    aa = zz * (1 - core) + xx * core
    bb = xx * (1 - core) + zz * core

    def at(r, s):
        return lax.rem(aa + r, 4) * sa + lax.rem(bb + s, 4) * sb

    def tp_at(dy, dc):
        return 2 * lax.rem(yy + dy, 4) + (core + dc - 2 * core * dc)

    def near(r, s):
        return {"kv": at(r, s), "tp": tp}

    local = []

    def fetch(src, dst):
        copy = pltpu.make_async_copy(src, dst, l_sem.at[len(local)])
        copy.start()
        local.append(copy)
        return copy

    w_in = [fetch(h, wst.at[pl.ds(64 * k, 64)]) for k, h in enumerate((wsk_hbm, wsv_hbm, wck_hbm, wcv_hbm))]
    tiles = TOK // TILE

    def tok_in(t):
        return fetch(tok_hbm.at[pl.ds(t * TILE, TILE)], tok.at[pl.ds(t * TILE, TILE)])

    t_in = [tok_in(0)]
    base = pl.ds(pl.multiple_of(kv * 32, 32), 32)
    a_in = [fetch(cc_hbm.at[base], ccv), fetch(cs_hbm.at[base], csv)]
    t_in += [tok_in(1), tok_in(2), tok_in(3)]
    q_in = [fetch(wq_hbm, wqv), fetch(bw_hbm, bwv)]
    i_in = [fetch(ki_hbm, kiv), fetch(vi_hbm, viv)]
    ow_in = fetch(ow_hbm, ow)

    barrier = pltpu.get_barrier_semaphore()
    peers = [near(r, 0) for r in (1, 2, 3)] + [near(0, s) for s in (1, 2, 3)]
    peers += [{"kv": kv, "tp": tp_at(*o)} for o in ORDER[:-1]]
    for peer in peers:
        pl.semaphore_signal(barrier, inc=1, device_id=peer, device_id_type=MESH)

    started = []

    def remote(src, dst, ssem, rsem, dev):
        return pltpu.make_async_remote_copy(
            src_ref=src, dst_ref=dst, send_sem=ssem, recv_sem=rsem, device_id=dev, device_id_type=MESH
        )

    def go(copy):
        copy.start()
        started.append(copy)

    half = NB // 2

    def a_copy(slot, part, r):
        rows = pl.ds(part * half, half)
        i = (slot // 2) * 2 + part
        return remote(kvb.at[rows], full[slot].at[rows], a_send.at[i], a_recv.at[i], near(r, 0))

    def af_copy(slot, part, r):
        rows = pl.ds(part * half, half)
        return remote(full[slot].at[rows], full2.at[rows], af_send.at[part], af_recv.at[part], near(r, 0))

    picks = picks_ref[...]
    code = (picks & (NB - 1)) + jnp.where(picks < 2 * lanes((8, 256)), 64, 0)
    for span in range(16):
        tabv[span:span + 1, :] = jnp.sum(jnp.where((picks >> 5) == span, code, 0), axis=0, keepdims=True)
    tab_in = fetch(tabv, tab)

    gain = gain_ref[...].astype(F32).reshape(1, D)
    for copy in w_in:
        copy.wait()
    for k in range(0, 256, 64):
        w1[k:k + 64, :] = (wst[k:k + 64, :].astype(F32) * gain).astype(BF)
    low = lanes((QB, 128)) < HD
    low64 = lanes((64, 128)) < HD
    front = (lanes((QB, 128)) % 64) < 32

    def turn(v, rows):
        other = jnp.where(front, pltpu.roll(v, 96, 1), pltpu.roll(v, 32, 1))
        return v * cos_s[rows, :] + other * sin_s[rows, :]

    embed = jnp.concatenate([ke_ref[...], ve_ref[...]], axis=1).astype(F32)
    embed = jnp.concatenate([embed] * (QB // CMP), axis=0)
    for t in range(tiles):
        t_in[t].wait()
        if t == 0:
            for copy in a_in:
                copy.wait()
        rows = pl.ds(t * TILE, TILE)
        x = tok[rows, :]
        proj = lax.dot_general(x, w1[...], NT, preferred_element_type=F32)
        xf = x.astype(F32)
        inv = lax.rsqrt(jnp.mean(xf * xf, axis=1, keepdims=True) + EPS)
        inv = jnp.broadcast_to(inv, (TILE, 128))
        inv_s[rows, :] = inv
        for j in range(TILE // QB):
            part = pl.ds(t * TILE + j * QB, QB)
            for u in (0, 1):
                g = t * (TILE // 64) + 2 * j + u
                cc, cs = ccv[g:g + 1, :], csv[g:g + 1, :]
                cos_s[pl.ds(g * 64, 64), :] = cc * fc_ref[...] - cs * fs_ref[...]
                sin_s[pl.ds(g * 64, 64), :] = (cs * fc_ref[...] + cc * fs_ref[...]) * sg_ref[...]
            scale = inv[j * QB:(j + 1) * QB]
            sel = proj[j * QB:(j + 1) * QB, 0:128] * scale
            sel = jnp.where(low, turn(sel, part), sel)
            vt = sel.T[64:128]
            b = t * (TILE // SEL) + 2 * j
            kvb[b] = jnp.where(low64, sel[0:64], pltpu.roll(vt, 64, 1)).astype(BF)
            kvb[b + 1] = jnp.where(low64, sel[64:128], vt).astype(BF)
            val = (proj[j * QB:(j + 1) * QB, 128:256] * scale).astype(BF).astype(F32) + embed
            val = val.astype(BF).astype(F32)
            for n in range(QB // CMP):
                spot = (t * (TILE // CMP) + j * (QB // CMP) + n) * PITCH
                raw[spot:spot + CMP, :] = val[n * CMP:(n + 1) * CMP]
        if t % 2 == 1:
            if t == 1:
                pl.semaphore_wait(barrier, len(peers))
            for slot, r in ((3, 1), (1, 3)):
                go(a_copy(slot, t // 2, r))

    def dest_of(c):
        dest = 0
        for k in range(8):
            dest = dest + jnp.where(c == k, tp_at(*ORDER[k]), 0)
        return dest

    def select(r, g):
        span = at(r, 0)
        dests = [at(0, s) for s in range(4)]

        def body(c, _):
            q0 = dest_of(c) * 2
            for k in (0, 1):
                for s in range(4):
                    blk = tab[span, dests[s] * 16 + q0 + k] & (NB - 1)
                    val = full[r][blk]
                    if s == 0:
                        inb[r, 0, 2 * c + k] = val
                    else:
                        outb[r, s - 1, 2 * c + k] = val
            return 0

        lax.fori_loop(4 * g, 4 * g + 4, body, 0)

    def f_copy(r, g, k):
        part = pl.ds(8 * g + 4 * k, 4)
        return remote(
            outb.at[r, 1, part], fwd.at[r, g, k], f_send.at[r, 2 * g + k], f_recv.at[r, 2 * g + k],
            near(0, 1 + 2 * k),
        )

    def b_copy(r, g, k):
        part = pl.ds(8 * g, 8)
        return remote(
            outb.at[r, 2 * k, part], inb.at[r, 3 - 2 * k, part], b_send.at[r, g, k], b_recv.at[r, g, k],
            near(0, 1 + 2 * k),
        )

    def bf_copy(r, g, k):
        part = pl.ds(8 * g + 4 * k, 4)
        return remote(
            fwd.at[r, g, k], inb.at[r, 2, part], b_send.at[r, g, 2 + k], b_recv.at[r, g, 2 + k],
            near(0, 1 + 2 * k),
        )

    def f_start(r, g):
        for k in (0, 1):
            go(f_copy(r, g, k))

    def d_start(r, g):
        for k in (0, 1):
            go(b_copy(r, g, k))

    def b_start(r, g):
        f_start(r, g)
        d_start(r, g)

    def b_forward(r, g):
        for k in (0, 1):
            f_copy(r, g, k).wait_recv()
            go(bf_copy(r, g, k))

    def b_wait(r, g):
        for k in (0, 1):
            b_copy(r, g, k).wait_recv()
            bf_copy(r, g, k).wait_recv()

    tab_in.wait()
    for g in (0, 1):
        select(0, g)
        f_start(0, g)
    d_start(0, 0)
    d_start(0, 1)

    for copy in i_in:
        copy.wait()
    keys, values = [], []
    for r in range(0, CMP, 2):
        one = raw[pl.ds(r, 64, stride=PITCH), :]
        two = raw[pl.ds(r + 1, 64, stride=PITCH), :]
        keys.append(jnp.where(low64, one, pltpu.roll(two, 64, 1)).astype(BF))
        values.append(jnp.where(low64, pltpu.roll(one, 64, 1), two).astype(BF))
    parts = []
    for rows, inner, outer in ((keys, kiv, ko_ref), (values, viv, vo_ref)):
        flat = jnp.concatenate(rows, axis=1)
        hidden = gelu(lax.dot_general(flat, inner[...], NT, preferred_element_type=F32)).astype(BF)
        parts.append(jnp.dot(hidden, outer[...], preferred_element_type=F32))
    both = jnp.concatenate(parts, axis=1)
    own[...] = jnp.where(low64, both, jnp.concatenate([both, both], axis=0).T[64:128]).astype(BF)
    sums[0, 0] = own[...]

    def s_copy(r):
        return remote(own, sums.at[0, 4 - r], s_send.at[r - 1], s_recv.at[3 - r], near(r, 0))

    def s_bundle(s):
        return remote(sums.at[0], sums.at[4 - s], s_send.at[2 + s], s_recv.at[6 - s], near(0, s))

    for r in (1, 2, 3):
        go(s_copy(r))

    a_copy(3, 0, 1).wait_recv()
    go(af_copy(3, 0, 1))

    for copy in q_in:
        copy.wait()
    w2[0:128, :] = (wqv[...].T.astype(F32) * gain).astype(BF)
    row = rows_of((128, 16))
    col = lanes((128, 16))
    e0 = jnp.where((row < 2) & (col == 2 * tp + row), 1.0, 0.0).astype(BF)
    e1 = jnp.where((row >= 2) & (row < 4) & (col == 2 * tp + row - 2), 1.0, 0.0).astype(BF)
    picked = jnp.dot(e0, bwv[0], preferred_element_type=F32) + jnp.dot(e1, bwv[1], preferred_element_type=F32)
    w2[128:256, :] = (picked * gain).astype(BF)
    zero = jnp.zeros((64, 256), BF)

    def queries(t):
        rows = pl.ds(t * TILE, TILE)
        proj = lax.dot_general(tok[rows, :], w2[...], NT, preferred_element_type=F32)
        for j in range(TILE // QB):
            part = pl.ds(t * TILE + j * QB, QB)
            q = t * (TILE // QB) + j
            scale = inv_s[part, :]
            v = proj[j * QB:(j + 1) * QB, 0:128] * scale
            for ref, val in ((qc, v), (qs, turn(v, part))):
                val = (val.T.astype(BF).astype(F32) * 0.125).astype(BF)
                ref[q, 0:64, 0:128] = val[0:64]
                ref[q, 0:64, 128:256] = val[64:128]
                ref[q, 64:128, :] = zero
            g = proj[j * QB:(j + 1) * QB, 128:256] * scale
            gt[q] = 1.0 / (1.0 + jnp.exp(-g.T[0:8]))

    queries(0)
    queries(1)
    a_copy(1, 1, 1).wait_recv()
    go(af_copy(1, 1, 3))
    for r in (1, 2, 3):
        s_copy(r).wait_recv()
    for s in (1, 2, 3):
        go(s_bundle(s))
    queries(2)
    queries(3)
    b_forward(0, 0)
    b_forward(0, 1)
    a_copy(3, 1, 1).wait_recv()
    a_copy(1, 0, 1).wait_recv()
    for g in (0, 1):
        for r in (3, 1):
            select(r, g)
            f_start(r, g)
    d_start(3, 0)
    d_start(1, 0)

    def values_of(blocks):
        pairs = [
            jnp.concatenate([blocks[k][:, HD:], blocks[k + 1][:, HD:]], axis=1) for k in range(0, len(blocks), 2)
        ]
        vt = jnp.concatenate(pairs, axis=1)
        return jnp.concatenate([vt, jnp.ones((16, vt.shape[1]), BF)], axis=0)

    def top(s):
        return jnp.max(s, axis=0, keepdims=True)

    def own_group(g):
        ids = [(tp_at(*ORDER[c]) * 2 + k, 2 * c + k) for c in range(4 * g, 4 * g + 4) for k in (0, 1)]
        blocks = [[kvb[2 * q], kvb[2 * q + 1]] for q, _ in ids]
        scs = [
            jnp.dot(jnp.concatenate(blk, axis=0), qs[q], preferred_element_type=F32)
            for blk, (q, _) in zip(blocks, ids)
        ]
        ps = []
        for sc, (_, i) in zip(scs, ids):
            sc = jnp.where(rows_of(sc.shape) <= (lanes(sc.shape) & (QB - 1)), sc, NEG)
            m = top(sc)
            mrow[i] = m
            ps.append(jnp.exp(sc - m).astype(BF))
        for p, blk, (_, i) in zip(ps, blocks, ids):
            acc[i] = jnp.dot(values_of(blk), p, preferred_element_type=F32)

    def far_steps(ids, r):
        blocks = [[inb[r, s, i] for s in range(4)] for _, i in ids]
        scs = [
            jnp.dot(jnp.concatenate(blk, axis=0), qs[q], preferred_element_type=F32)
            for blk, (q, _) in zip(blocks, ids)
        ]
        ms, ps, scale = [], [], []
        for sc, (q, i) in zip(scs, ids):
            m = old = mrow[i]
            bias = []
            for s in range(4):
                used = lax.shift_right_logical(tab[at(r, s), kv * 16 + q], 6)
                bias.append((used.astype(F32) - 1.0) * 1e30)
                m = jnp.maximum(m, top(sc[64 * s:64 * s + 64]) + bias[s])
            p = [jnp.exp(sc[64 * s:64 * s + 64] - (m - bias[s])).astype(BF) for s in range(4)]
            ms.append(m)
            ps.append(jnp.concatenate(p, axis=0))
            scale.append(jnp.exp(old - m))
        adds = [jnp.dot(values_of(blk), p, preferred_element_type=F32) for blk, p in zip(blocks, ps)]
        return ms, [acc[i] * sc + add for (_, i), sc, add in zip(ids, scale, adds)]

    def ids_of(c0, n):
        return [(tp_at(*ORDER[c]) * 2 + k, 2 * c + k) for c in range(c0, c0 + n) for k in (0, 1)]

    def far_loop(g, lo, hi):
        ids = ids_of(4 * g, 4)

        def body(n, _):
            ms, accs = far_steps(ids, n + n // 2)
            for (_, i), m, a in zip(ids, ms, accs):
                mrow[i] = m
                acc[i] = a
            return 0

        lax.fori_loop(lo, hi, body, 0)

    def compressed(n, _):
        ids = []
        for c in (n,):
            q0 = dest_of(c) * 2
            ids += [(q0 + k, 2 * c + k) for k in (0, 1)]
        scs = [
            [jnp.dot(sums[s].reshape(256, 128), qc[q], preferred_element_type=F32) for s in range(4)] for q, _ in ids
        ]
        ps = []
        for (q, _), sc in zip(ids, scs):
            ones, ms = [], []
            m = jnp.full((1, 256), FLOOR, F32)
            for s in range(4):
                for r in range(4):
                    one = sc[s][64 * r:64 * r + 64]
                    bias = jnp.where(at(r, s) < kv, 0.0, NEG)
                    if r == 0 and s == 0:
                        end = (rows_of(one.shape) + 1) * CMP - 1
                        one = jnp.where(end <= q * QB + (lanes(one.shape) & (QB - 1)), one, NEG)
                        bias = 0.0
                    ones.append(one)
                    ms.append(bias)
                    m = jnp.maximum(m, top(one) + bias)
            ps.append(jnp.concatenate([jnp.exp(o - (m - b)).astype(BF) for o, b in zip(ones, ms)], axis=0))
        for (_, i), p in zip(ids, ps):
            total = jnp.dot(vtc[...], p, preferred_element_type=F32)
            den = total[64:65]
            ocmp[i] = jnp.where(den > 0, total[0:64] / jnp.maximum(den, 1e-30), 0.0)
        return 0

    def finish(c0, n):
        ids = ids_of(c0, n)
        _, accs = far_steps(ids, 2)
        for (q, i), a in zip(ids, accs):
            o = a[0:64] / a[64:65]
            oc = ocmp[i]
            g = gt[q]
            heads = [
                g[h:h + 1] * oc[:, 128 * h:128 * h + 128] + g[2 + h:3 + h] * o[:, 128 * h:128 * h + 128]
                for h in (0, 1)
            ]
            mix[i // 2, (i % 2) * QB:(i % 2 + 1) * QB, :] = jnp.concatenate(heads, axis=0).T.astype(BF)

    def t_copy(c, slot):
        return remote(mix.at[c], hr.at[slot], t_send.at[c], t_recv.at[c], {"kv": kv, "tp": tp_at(*ORDER[c])})

    own_group(0)
    own_group(1)
    af_copy(3, 0, 1).wait_recv()
    af_copy(1, 1, 1).wait_recv()
    for g in (0, 1):
        select(2, g)
        f_start(2, g)
    b_forward(3, 0)
    b_forward(1, 0)
    d_start(2, 0)
    for s in (1, 2, 3):
        s_bundle(s).wait_recv()
    for s in range(4):
        vtc[:, 256 * s:256 * s + 256] = values_of([sums[s, r] for r in range(4)])
    lax.fori_loop(0, 2, compressed, 0)
    b_forward(2, 0)
    b_forward(3, 1)
    b_forward(1, 1)
    for r in (3, 1, 2):
        d_start(r, 1)
    lax.fori_loop(2, 4, compressed, 0)
    b_forward(2, 1)
    lax.fori_loop(4, 8, compressed, 0)
    for g in (0, 1):
        b_wait(0, g)
        far_loop(g, 0, 1)
    for g in (0, 1):
        for r in (3, 1):
            b_wait(r, g)
        far_loop(g, 1, 3)
        b_wait(2, g)
        for c in (4 * g, 4 * g + 2):
            finish(c, 2)
            for k in (c, c + 1):
                if k < 7:
                    go(t_copy(k, tp))
    hr[tp] = mix[7]

    ow_in.wait()
    for c in range(7):
        dy, dc = ORDER[c]
        t_copy(c, tp_at((4 - dy) % 4, dc)).wait_recv()
    x = jnp.concatenate([hr[t] for t in range(8)], axis=1)
    outs = []
    for n in range(4):
        cols = pl.ds(n * 512, 512)
        res[:, cols] = jnp.dot(x, ow[:, cols], preferred_element_type=F32).astype(BF)
        copy = pltpu.make_async_copy(res.at[:, cols], out_hbm.at[:, cols], o_sem.at[n])
        copy.start()
        outs.append(copy)
    for copy in started:
        copy.wait_send()
    for copy in outs:
        copy.wait()


def per_device(
    tokens, norm_gain, query_weight, cmp_key_weight, cmp_value_weight, sel_key_weight, sel_value_weight,
    branch_weight, key_embed, key_inner, key_outer, value_embed, value_inner, value_outer, out_weight, chosen,
):
    cc, cs, fc, fs, sg = angle_tables()
    vm = pl.BlockSpec(memory_space=pltpu.VMEM)
    hbm = pl.BlockSpec(memory_space=pl.ANY)
    dma = pltpu.SemaphoreType.DMA
    v = pltpu.VMEM
    return pl.pallas_call(
        kernel,
        in_specs=[vm] * 9 + [hbm] * 12,
        out_specs=hbm,
        out_shape=jax.ShapeDtypeStruct((256, D), BF),
        scratch_shapes=[
            pltpu.SMEM((16, 256), jnp.int32), v((16, 256), jnp.int32),
            v((TOK, D), BF), v((256, D), BF), v((256, D), BF), v((D, 128), BF), v((2, 16, D), BF), v((256, D), BF),
            v((64, D), BF), v((64, D), BF), v((32, 128), F32), v((32, 128), F32), v((1024, D), BF),
            v((TOK, 128), F32), v((TOK, 128), F32), v((TOK, 128), F32), v((64 * PITCH, 128), F32),
            v((NQ, 128, 256), BF), v((NQ, 128, 256), BF), v((NQ, 8, 128), F32),
            v((NB, SEL, 128), BF), v((NB, SEL, 128), BF), v((NB, SEL, 128), BF), v((NB, SEL, 128), BF),
            v((4, 4, NQ, SEL, 128), BF), v((4, 3, NQ, SEL, 128), BF), v((4, 2, 2, 4, SEL, 128), BF),
            v((64, 128), BF), v((4, 4, 64, 128), BF), v((80, 1024), BF),
            v((NQ, 80, 256), F32), v((NQ, 1, 256), F32), v((NQ, 64, 256), F32),
            v((8, 256, 128), BF), v((8, 256, 128), BF), v((256, D), BF),
            dma((17,)), dma((4,)), dma((4,)), dma((2,)), dma((2,)), dma((6,)), dma((6,)),
            dma((4, 2, 4)), dma((4, 2, 4)), dma((4, 4)), dma((4, 4)), dma((8,)), dma((8,)), dma((4,)),
        ],
        compiler_params=pltpu.CompilerParams(collective_id=0, has_side_effects=True, vmem_limit_bytes=67043328),
        name="layer",
    )(
        chosen[0].T, norm_gain, key_embed[0], key_outer[0], value_embed[0], value_outer[0], fc, fs, sg,
        tokens, query_weight, cmp_key_weight.T, cmp_value_weight.T, sel_key_weight.T, sel_value_weight.T,
        branch_weight.transpose(0, 2, 1), key_inner[0].T, value_inner[0].T, cc, cs, out_weight,
    )


def solution(mesh):
    placed = (
        P("kv", None), P(), P(None, "tp"), P(None, "tp"), P(None, "tp"), P(None, "tp"), P(None, "tp"), P(),
        P("tp", None, None), P("tp", None, None), P("tp", None, None), P("tp", None, None),
        P("tp", None, None), P("tp", None, None), P(), P("tp", None, None),
    )
    return jax.shard_map(
        per_device, mesh=mesh, in_specs=placed, out_specs=P(("kv", "tp"), None), check_vma=False
    )
```

```python
import jax
import jax.numpy as jnp
import numpy as np
from jax import lax
from jax.experimental import pallas as pl
from jax.experimental.pallas import tpu as pltpu
from jax.sharding import PartitionSpec as P

D = 2048
HD = 64
CMP = 32
SEL = 64
QB = 128
TOK = 2048
NQ = TOK // QB
NB = TOK // SEL
PITCH = 40
EPS = 1e-06
NEG = -1e30
FLOOR = -1e20
TILE = 512
MESH = pl.DeviceIdType.MESH
NT = (((1,), (1,)), ((), ()))
BF = jnp.bfloat16
F32 = jnp.float32
ORDER = ((2, 0), (2, 1), (1, 0), (3, 0), (1, 1), (3, 1), (0, 1), (0, 0))


def angle_tables():
    lane = np.arange(128)
    freq = 10000.0 ** (-(lane % 32) / 32.0)
    sign = np.where(lane % 64 < 32, -1.0, 1.0)
    coarse = np.arange(512)[:, None] * 64.0 * freq
    fine = np.arange(64)[:, None] * freq
    as32 = lambda t: jnp.asarray(np.asarray(t, np.float32))
    return as32(np.cos(coarse)), as32(np.sin(coarse)), as32(np.cos(fine)), as32(np.sin(fine)), as32(sign[None])


def lanes(shape):
    return lax.broadcasted_iota(jnp.int32, shape, 1)


def rows_of(shape):
    return lax.broadcasted_iota(jnp.int32, shape, 0)


def gelu(x):
    return 0.5 * x * (1.0 + jnp.tanh(0.7978845608028654 * (x + 0.044715 * (x * x * x))))


def kernel(
    picks_ref, gain_ref, ke_ref, ko_ref, ve_ref, vo_ref, fc_ref, fs_ref, sg_ref,
    tok_hbm, wq_hbm, wck_hbm, wcv_hbm, wsk_hbm, wsv_hbm, bw_hbm, ki_hbm, vi_hbm, cc_hbm, cs_hbm, ow_hbm,
    out_hbm,
    tab, tabv, tok, wst, w1, wqv, bwv, w2, kiv, viv, ccv, csv, ow, inv_s, cos_s, sin_s, raw, qs, qc, gt,
    kvb, full1, full2, full3, inb, outb, fwd, own, sums, vtc, acc, mrow, ocmp, mix, hr, res, part_s,
    l_sem, a_send, a_recv, af_send, af_recv, s_send, s_recv, b_send, b_recv, f_send, f_recv, t_send, t_recv, o_sem,
):
    full = (kvb, full1, full2, full3)
    tp = lax.axis_index("tp")
    kv = lax.axis_index("kv")
    core = lax.rem(tp, 2)
    yy = tp // 2
    zz = kv // 4
    xx = lax.rem(kv, 4)
    sa = 4 - 3 * core
    sb = 1 + 3 * core
    aa = zz * (1 - core) + xx * core
    bb = xx * (1 - core) + zz * core

    def at(r, s):
        return lax.rem(aa + r, 4) * sa + lax.rem(bb + s, 4) * sb

    def tp_at(dy, dc):
        return 2 * lax.rem(yy + dy, 4) + (core + dc - 2 * core * dc)

    def near(r, s):
        return {"kv": at(r, s), "tp": tp}

    local = []

    def fetch(src, dst):
        copy = pltpu.make_async_copy(src, dst, l_sem.at[len(local)])
        copy.start()
        local.append(copy)
        return copy

    w_in = [fetch(h, wst.at[pl.ds(64 * k, 64)]) for k, h in enumerate((wsk_hbm, wsv_hbm, wck_hbm, wcv_hbm))]
    tiles = TOK // TILE

    def tok_in(t):
        return fetch(tok_hbm.at[pl.ds(t * TILE, TILE)], tok.at[pl.ds(t * TILE, TILE)])

    t_in = [tok_in(0)]
    base = pl.ds(pl.multiple_of(kv * 32, 32), 32)
    a_in = [fetch(cc_hbm.at[base], ccv), fetch(cs_hbm.at[base], csv)]
    t_in += [tok_in(1), tok_in(2), tok_in(3)]
    q_in = [fetch(wq_hbm, wqv), fetch(bw_hbm, bwv)]
    i_in = [fetch(ki_hbm, kiv), fetch(vi_hbm, viv)]
    ow_in = fetch(ow_hbm, ow)

    barrier = pltpu.get_barrier_semaphore()
    peers = [near(r, 0) for r in (1, 2, 3)] + [near(0, s) for s in (1, 2, 3)]
    peers += [{"kv": kv, "tp": tp_at(*o)} for o in ORDER[:-1]]
    for peer in peers:
        pl.semaphore_signal(barrier, inc=1, device_id=peer, device_id_type=MESH)

    started = []

    def remote(src, dst, ssem, rsem, dev):
        return pltpu.make_async_remote_copy(
            src_ref=src, dst_ref=dst, send_sem=ssem, recv_sem=rsem, device_id=dev, device_id_type=MESH
        )

    def go(copy):
        copy.start()
        started.append(copy)

    half = NB // 2

    def a_copy(slot, part, r):
        rows = pl.ds(part * half, half)
        i = (slot // 2) * 2 + part
        return remote(kvb.at[rows], full[slot].at[rows], a_send.at[i], a_recv.at[i], near(r, 0))

    def af_copy(slot, part, r):
        rows = pl.ds(part * half, half)
        return remote(full[slot].at[rows], full2.at[rows], af_send.at[part], af_recv.at[part], near(r, 0))

    picks = picks_ref[...]
    code = (picks & (NB - 1)) + jnp.where(picks < 2 * lanes((8, 256)), 64, 0)
    for span in range(16):
        tabv[span:span + 1, :] = jnp.sum(jnp.where((picks >> 5) == span, code, 0), axis=0, keepdims=True)
    tab_in = fetch(tabv, tab)

    gain = gain_ref[...].astype(F32).reshape(1, D)
    for copy in w_in:
        copy.wait()
    for k in range(0, 256, 64):
        w1[k:k + 64, :] = (wst[k:k + 64, :].astype(F32) * gain).astype(BF)
    low = lanes((QB, 128)) < HD
    low64 = lanes((64, 128)) < HD
    front = (lanes((QB, 128)) % 64) < 32

    def turn(v, rows):
        other = jnp.where(front, pltpu.roll(v, 96, 1), pltpu.roll(v, 32, 1))
        return v * cos_s[rows, :] + other * sin_s[rows, :]

    embed = jnp.concatenate([ke_ref[...], ve_ref[...]], axis=1).astype(F32)
    embed = jnp.concatenate([embed] * (QB // CMP), axis=0)
    for t in range(tiles):
        t_in[t].wait()
        if t == 0:
            for copy in a_in:
                copy.wait()
        rows = pl.ds(t * TILE, TILE)
        x = tok[rows, :]
        proj = lax.dot_general(x, w1[...], NT, preferred_element_type=F32)
        xf = x.astype(F32)
        inv = lax.rsqrt(jnp.mean(xf * xf, axis=1, keepdims=True) + EPS)
        inv = jnp.broadcast_to(inv, (TILE, 128))
        inv_s[rows, :] = inv
        for j in range(TILE // QB):
            part = pl.ds(t * TILE + j * QB, QB)
            for u in (0, 1):
                g = t * (TILE // 64) + 2 * j + u
                cc, cs = ccv[g:g + 1, :], csv[g:g + 1, :]
                cos_s[pl.ds(g * 64, 64), :] = cc * fc_ref[...] - cs * fs_ref[...]
                sin_s[pl.ds(g * 64, 64), :] = (cs * fc_ref[...] + cc * fs_ref[...]) * sg_ref[...]
            scale = inv[j * QB:(j + 1) * QB]
            sel = proj[j * QB:(j + 1) * QB, 0:128] * scale
            sel = jnp.where(low, turn(sel, part), sel)
            vt = sel.T[64:128]
            b = t * (TILE // SEL) + 2 * j
            kvb[b] = jnp.where(low64, sel[0:64], pltpu.roll(vt, 64, 1)).astype(BF)
            kvb[b + 1] = jnp.where(low64, sel[64:128], vt).astype(BF)
            val = (proj[j * QB:(j + 1) * QB, 128:256] * scale).astype(BF).astype(F32) + embed
            val = val.astype(BF).astype(F32)
            for n in range(QB // CMP):
                spot = (t * (TILE // CMP) + j * (QB // CMP) + n) * PITCH
                raw[spot:spot + CMP, :] = val[n * CMP:(n + 1) * CMP]
        if t % 2 == 1:
            if t == 1:
                pl.semaphore_wait(barrier, len(peers))
            for slot, r in ((3, 1), (1, 3)):
                go(a_copy(slot, t // 2, r))

    def dest_of(c):
        dest = 0
        for k in range(8):
            dest = dest + jnp.where(c == k, tp_at(*ORDER[k]), 0)
        return dest

    def select(r, g):
        span = at(r, 0)
        dests = [at(0, s) for s in range(4)]

        def body(c, _):
            q0 = dest_of(c) * 2
            for k in (0, 1):
                for s in range(4):
                    blk = tab[span, dests[s] * 16 + q0 + k] & (NB - 1)
                    val = full[r][blk]
                    if s == 0:
                        inb[r, 0, 2 * c + k] = val
                    else:
                        outb[r, s - 1, 2 * c + k] = val
            return 0

        lax.fori_loop(4 * g, 4 * g + 4, body, 0)

    def f_copy(r, g, k):
        part = pl.ds(8 * g + 4 * k, 4)
        return remote(
            outb.at[r, 1, part], fwd.at[r, g, k], f_send.at[r, 2 * g + k], f_recv.at[r, 2 * g + k],
            near(0, 1 + 2 * k),
        )

    def b_copy(r, g, k):
        part = pl.ds(8 * g, 8)
        return remote(
            outb.at[r, 2 * k, part], inb.at[r, 3 - 2 * k, part], b_send.at[r, g, k], b_recv.at[r, g, k],
            near(0, 1 + 2 * k),
        )

    def bf_copy(r, g, k):
        part = pl.ds(8 * g + 4 * k, 4)
        return remote(
            fwd.at[r, g, k], inb.at[r, 2, part], b_send.at[r, g, 2 + k], b_recv.at[r, g, 2 + k],
            near(0, 1 + 2 * k),
        )

    def f_start(r, g):
        for k in (0, 1):
            go(f_copy(r, g, k))

    def d_start(r, g):
        for k in (0, 1):
            go(b_copy(r, g, k))

    def b_start(r, g):
        f_start(r, g)
        d_start(r, g)

    def b_forward(r, g):
        for k in (0, 1):
            f_copy(r, g, k).wait_recv()
            go(bf_copy(r, g, k))

    def b_wait(r, g):
        for k in (0, 1):
            b_copy(r, g, k).wait_recv()
            bf_copy(r, g, k).wait_recv()

    tab_in.wait()
    for g in (0, 1):
        select(0, g)
        f_start(0, g)
    d_start(0, 0)
    d_start(0, 1)

    for copy in i_in:
        copy.wait()
    keys, values = [], []
    for r in range(0, CMP, 2):
        one = raw[pl.ds(r, 64, stride=PITCH), :]
        two = raw[pl.ds(r + 1, 64, stride=PITCH), :]
        keys.append(jnp.where(low64, one, pltpu.roll(two, 64, 1)).astype(BF))
        values.append(jnp.where(low64, pltpu.roll(one, 64, 1), two).astype(BF))
    parts = []
    for rows, inner, outer in ((keys, kiv, ko_ref), (values, viv, vo_ref)):
        flat = jnp.concatenate(rows, axis=1)
        hidden = gelu(lax.dot_general(flat, inner[...], NT, preferred_element_type=F32)).astype(BF)
        parts.append(jnp.dot(hidden, outer[...], preferred_element_type=F32))
    both = jnp.concatenate(parts, axis=1)
    own[...] = jnp.where(low64, both, jnp.concatenate([both, both], axis=0).T[64:128]).astype(BF)
    sums[0, 0] = own[...]

    def s_copy(r):
        return remote(own, sums.at[0, 4 - r], s_send.at[r - 1], s_recv.at[3 - r], near(r, 0))

    def s_bundle(s):
        return remote(sums.at[0], sums.at[4 - s], s_send.at[2 + s], s_recv.at[6 - s], near(0, s))

    for r in (1, 2, 3):
        go(s_copy(r))

    a_copy(3, 0, 1).wait_recv()
    go(af_copy(3, 0, 1))

    for copy in q_in:
        copy.wait()
    w2[0:128, :] = (wqv[...].T.astype(F32) * gain).astype(BF)
    row = rows_of((128, 16))
    col = lanes((128, 16))
    e0 = jnp.where((row < 2) & (col == 2 * tp + row), 1.0, 0.0).astype(BF)
    e1 = jnp.where((row >= 2) & (row < 4) & (col == 2 * tp + row - 2), 1.0, 0.0).astype(BF)
    picked = jnp.dot(e0, bwv[0], preferred_element_type=F32) + jnp.dot(e1, bwv[1], preferred_element_type=F32)
    w2[128:256, :] = (picked * gain).astype(BF)
    zero = jnp.zeros((64, 256), BF)

    def queries(t):
        rows = pl.ds(t * TILE, TILE)
        proj = lax.dot_general(tok[rows, :], w2[...], NT, preferred_element_type=F32)
        for j in range(TILE // QB):
            part = pl.ds(t * TILE + j * QB, QB)
            q = t * (TILE // QB) + j
            scale = inv_s[part, :]
            v = proj[j * QB:(j + 1) * QB, 0:128] * scale
            for ref, val in ((qc, v), (qs, turn(v, part))):
                val = (val.T.astype(BF).astype(F32) * 0.125).astype(BF)
                ref[q, 0:64, 0:128] = val[0:64]
                ref[q, 0:64, 128:256] = val[64:128]
                ref[q, 64:128, :] = zero
            g = proj[j * QB:(j + 1) * QB, 128:256] * scale
            gt[q] = 1.0 / (1.0 + jnp.exp(-g.T[0:8]))

    queries(0)
    queries(1)
    a_copy(1, 1, 1).wait_recv()
    go(af_copy(1, 1, 3))
    for r in (1, 2, 3):
        s_copy(r).wait_recv()
    for s in (1, 2, 3):
        go(s_bundle(s))
    queries(2)
    queries(3)
    b_forward(0, 0)
    b_forward(0, 1)
    a_copy(3, 1, 1).wait_recv()
    a_copy(1, 0, 1).wait_recv()
    for g in (0, 1):
        for r in (3, 1):
            select(r, g)
            f_start(r, g)
    d_start(3, 0)
    d_start(1, 0)

    def values_of(blocks):
        pairs = [
            jnp.concatenate([blocks[k][:, HD:], blocks[k + 1][:, HD:]], axis=1) for k in range(0, len(blocks), 2)
        ]
        vt = jnp.concatenate(pairs, axis=1)
        return jnp.concatenate([vt, jnp.ones((16, vt.shape[1]), BF)], axis=0)

    def top(s):
        return jnp.max(s, axis=0, keepdims=True)

    def own_group(g):
        ids = [(tp_at(*ORDER[c]) * 2 + k, 2 * c + k) for c in range(4 * g, 4 * g + 4) for k in (0, 1)]
        blocks = [[kvb[2 * q], kvb[2 * q + 1]] for q, _ in ids]
        scs = [
            jnp.dot(jnp.concatenate(blk, axis=0), qs[q], preferred_element_type=F32)
            for blk, (q, _) in zip(blocks, ids)
        ]
        ps = []
        for sc, (_, i) in zip(scs, ids):
            sc = jnp.where(rows_of(sc.shape) <= (lanes(sc.shape) & (QB - 1)), sc, NEG)
            m = top(sc)
            mrow[i] = m
            ps.append(jnp.exp(sc - m).astype(BF))
        for p, blk, (_, i) in zip(ps, blocks, ids):
            acc[i] = jnp.dot(values_of(blk), p, preferred_element_type=F32)

    def far_steps(ids, r):
        blocks = [[inb[r, s, i] for s in range(4)] for _, i in ids]
        scs = [
            jnp.dot(jnp.concatenate(blk, axis=0), qs[q], preferred_element_type=F32)
            for blk, (q, _) in zip(blocks, ids)
        ]
        ms, ps, scale = [], [], []
        for sc, (q, i) in zip(scs, ids):
            m = old = mrow[i]
            bias = []
            for s in range(4):
                used = lax.shift_right_logical(tab[at(r, s), kv * 16 + q], 6)
                bias.append((used.astype(F32) - 1.0) * 1e30)
                m = jnp.maximum(m, top(sc[64 * s:64 * s + 64]) + bias[s])
            p = [jnp.exp(sc[64 * s:64 * s + 64] - (m - bias[s])).astype(BF) for s in range(4)]
            ms.append(m)
            ps.append(jnp.concatenate(p, axis=0))
            scale.append(jnp.exp(old - m))
        adds = [jnp.dot(values_of(blk), p, preferred_element_type=F32) for blk, p in zip(blocks, ps)]
        return ms, [acc[i] * sc + add for (_, i), sc, add in zip(ids, scale, adds)]

    def ids_of(c0, n):
        return [(tp_at(*ORDER[c]) * 2 + k, 2 * c + k) for c in range(c0, c0 + n) for k in (0, 1)]

    def far_loop(g, lo, hi):
        ids = ids_of(4 * g, 4)

        def body(n, _):
            ms, accs = far_steps(ids, n + n // 2)
            for (_, i), m, a in zip(ids, ms, accs):
                mrow[i] = m
                acc[i] = a
            return 0

        lax.fori_loop(lo, hi, body, 0)

    def compressed(n, _):
        ids = []
        for c in (n,):
            q0 = dest_of(c) * 2
            ids += [(q0 + k, 2 * c + k) for k in (0, 1)]
        scs = [
            [jnp.dot(sums[s].reshape(256, 128), qc[q], preferred_element_type=F32) for s in range(4)] for q, _ in ids
        ]
        ps = []
        for (q, _), sc in zip(ids, scs):
            ones, ms = [], []
            m = jnp.full((1, 256), FLOOR, F32)
            for s in range(4):
                for r in range(4):
                    one = sc[s][64 * r:64 * r + 64]
                    bias = jnp.where(at(r, s) < kv, 0.0, NEG)
                    if r == 0 and s == 0:
                        end = (rows_of(one.shape) + 1) * CMP - 1
                        one = jnp.where(end <= q * QB + (lanes(one.shape) & (QB - 1)), one, NEG)
                        bias = 0.0
                    ones.append(one)
                    ms.append(bias)
                    m = jnp.maximum(m, top(one) + bias)
            ps.append(jnp.concatenate([jnp.exp(o - (m - b)).astype(BF) for o, b in zip(ones, ms)], axis=0))
        for (_, i), p in zip(ids, ps):
            total = jnp.dot(vtc[...], p, preferred_element_type=F32)
            den = total[64:65]
            ocmp[i] = jnp.where(den > 0, total[0:64] / jnp.maximum(den, 1e-30), 0.0)
        return 0

    def finish(c0, n):
        ids = ids_of(c0, n)
        _, accs = far_steps(ids, 2)
        for (q, i), a in zip(ids, accs):
            o = a[0:64] / a[64:65]
            oc = ocmp[i]
            g = gt[q]
            heads = [
                g[h:h + 1] * oc[:, 128 * h:128 * h + 128] + g[2 + h:3 + h] * o[:, 128 * h:128 * h + 128]
                for h in (0, 1)
            ]
            mix[i // 2, (i % 2) * QB:(i % 2 + 1) * QB, :] = jnp.concatenate(heads, axis=0).T.astype(BF)

    def t_copy(c, slot):
        return remote(mix.at[c], hr.at[slot], t_send.at[c], t_recv.at[c], {"kv": kv, "tp": tp_at(*ORDER[c])})

    own_group(0)
    own_group(1)
    af_copy(3, 0, 1).wait_recv()
    af_copy(1, 1, 1).wait_recv()
    for g in (0, 1):
        select(2, g)
        f_start(2, g)
    b_forward(3, 0)
    b_forward(1, 0)
    d_start(2, 0)
    for s in (1, 2, 3):
        s_bundle(s).wait_recv()
    for s in range(4):
        vtc[:, 256 * s:256 * s + 256] = values_of([sums[s, r] for r in range(4)])
    lax.fori_loop(0, 3, compressed, 0)
    b_forward(2, 0)
    b_forward(3, 1)
    b_forward(1, 1)
    for r in (3, 1, 2):
        d_start(r, 1)
    lax.fori_loop(3, 5, compressed, 0)
    b_forward(2, 1)
    lax.fori_loop(5, 8, compressed, 0)
    for g in (0, 1):
        b_wait(0, g)
        far_loop(g, 0, 1)
    for g in (0, 1):
        for r in (3, 1):
            b_wait(r, g)
        far_loop(g, 1, 3)
        b_wait(2, g)
        for c in (4 * g, 4 * g + 2):
            finish(c, 2)
            for k in (c, c + 1):
                if k < 7:
                    go(t_copy(k, tp))
    hr[tp] = mix[7]

    ow_in.wait()

    def source(c):
        dy, dc = ORDER[c]
        return tp_at((4 - dy) % 4, dc)

    def arrive(c):
        t_copy(c, source(c)).wait_recv()

    def product(cs, cols):
        x = jnp.concatenate([hr[source(c)] for c in cs], axis=1)
        w = jnp.concatenate([ow[pl.ds(pl.multiple_of(source(c) * 128, 128), 128), cols] for c in cs], axis=0)
        return jnp.dot(x, w, preferred_element_type=F32)

    early, late = (7, 0, 1, 2, 3), (4, 5, 6)
    for c in early[1:]:
        arrive(c)
    for n in range(4):
        cols = pl.ds(n * 512, 512)
        part_s[:, cols] = product(early, cols)
    for c in late:
        arrive(c)
    outs = []
    for n in range(4):
        cols = pl.ds(n * 512, 512)
        res[:, cols] = (part_s[:, cols] + product(late, cols)).astype(BF)
        copy = pltpu.make_async_copy(res.at[:, cols], out_hbm.at[:, cols], o_sem.at[n])
        copy.start()
        outs.append(copy)
    for copy in started:
        copy.wait_send()
    for copy in outs:
        copy.wait()


def per_device(
    tokens, norm_gain, query_weight, cmp_key_weight, cmp_value_weight, sel_key_weight, sel_value_weight,
    branch_weight, key_embed, key_inner, key_outer, value_embed, value_inner, value_outer, out_weight, chosen,
):
    cc, cs, fc, fs, sg = angle_tables()
    vm = pl.BlockSpec(memory_space=pltpu.VMEM)
    hbm = pl.BlockSpec(memory_space=pl.ANY)
    dma = pltpu.SemaphoreType.DMA
    v = pltpu.VMEM
    return pl.pallas_call(
        kernel,
        in_specs=[vm] * 9 + [hbm] * 12,
        out_specs=hbm,
        out_shape=jax.ShapeDtypeStruct((256, D), BF),
        scratch_shapes=[
            pltpu.SMEM((16, 256), jnp.int32), v((16, 256), jnp.int32),
            v((TOK, D), BF), v((256, D), BF), v((256, D), BF), v((D, 128), BF), v((2, 16, D), BF), v((256, D), BF),
            v((64, D), BF), v((64, D), BF), v((32, 128), F32), v((32, 128), F32), v((1024, D), BF),
            v((TOK, 128), F32), v((TOK, 128), F32), v((TOK, 128), F32), v((64 * PITCH, 128), F32),
            v((NQ, 128, 256), BF), v((NQ, 128, 256), BF), v((NQ, 8, 128), F32),
            v((NB, SEL, 128), BF), v((NB, SEL, 128), BF), v((NB, SEL, 128), BF), v((NB, SEL, 128), BF),
            v((4, 4, NQ, SEL, 128), BF), v((4, 3, NQ, SEL, 128), BF), v((4, 2, 2, 4, SEL, 128), BF),
            v((64, 128), BF), v((4, 4, 64, 128), BF), v((80, 1024), BF),
            v((NQ, 80, 256), F32), v((NQ, 1, 256), F32), v((NQ, 64, 256), F32),
            v((8, 256, 128), BF), v((8, 256, 128), BF), v((256, D), BF), v((256, D), F32),
            dma((17,)), dma((4,)), dma((4,)), dma((2,)), dma((2,)), dma((6,)), dma((6,)),
            dma((4, 2, 4)), dma((4, 2, 4)), dma((4, 4)), dma((4, 4)), dma((8,)), dma((8,)), dma((4,)),
        ],
        compiler_params=pltpu.CompilerParams(collective_id=0, has_side_effects=True, vmem_limit_bytes=67043328),
        name="layer",
    )(
        chosen[0].T, norm_gain, key_embed[0], key_outer[0], value_embed[0], value_outer[0], fc, fs, sg,
        tokens, query_weight, cmp_key_weight.T, cmp_value_weight.T, sel_key_weight.T, sel_value_weight.T,
        branch_weight.transpose(0, 2, 1), key_inner[0].T, value_inner[0].T, cc, cs, out_weight,
    )


def solution(mesh):
    placed = (
        P("kv", None), P(), P(None, "tp"), P(None, "tp"), P(None, "tp"), P(None, "tp"), P(None, "tp"), P(),
        P("tp", None, None), P("tp", None, None), P("tp", None, None), P("tp", None, None),
        P("tp", None, None), P("tp", None, None), P(), P("tp", None, None),
    )
    return jax.shard_map(
        per_device, mesh=mesh, in_specs=placed, out_specs=P(("kv", "tp"), None), check_vma=False
    )
```

```python
import jax
import jax.numpy as jnp
import numpy as np
from jax import lax
from jax.experimental import pallas as pl
from jax.experimental.pallas import tpu as pltpu
from jax.sharding import PartitionSpec as P

D = 2048
HD = 64
CMP = 32
SEL = 64
QB = 128
TOK = 2048
NQ = TOK // QB
NB = TOK // SEL
PITCH = 40
EPS = 1e-06
NEG = -1e30
FLOOR = -1e20
TILE = 512
MESH = pl.DeviceIdType.MESH
NT = (((1,), (1,)), ((), ()))
BF = jnp.bfloat16
F32 = jnp.float32
ORDER = ((2, 0), (2, 1), (1, 0), (3, 0), (1, 1), (3, 1), (0, 1), (0, 0))


def angle_tables():
    lane = np.arange(128)
    freq = 10000.0 ** (-(lane % 32) / 32.0)
    sign = np.where(lane % 64 < 32, -1.0, 1.0)
    coarse = np.arange(512)[:, None] * 64.0 * freq
    fine = np.arange(64)[:, None] * freq
    as32 = lambda t: jnp.asarray(np.asarray(t, np.float32))
    return as32(np.cos(coarse)), as32(np.sin(coarse)), as32(np.cos(fine)), as32(np.sin(fine)), as32(sign[None])


def lanes(shape):
    return lax.broadcasted_iota(jnp.int32, shape, 1)


def rows_of(shape):
    return lax.broadcasted_iota(jnp.int32, shape, 0)


def gelu(x):
    return 0.5 * x * (1.0 + jnp.tanh(0.7978845608028654 * (x + 0.044715 * (x * x * x))))


def kernel(
    picks_ref, gain_ref, ke_ref, ko_ref, ve_ref, vo_ref, fc_ref, fs_ref, sg_ref,
    tok_hbm, wq_hbm, wck_hbm, wcv_hbm, wsk_hbm, wsv_hbm, bw_hbm, ki_hbm, vi_hbm, cc_hbm, cs_hbm, ow_hbm,
    out_hbm,
    tab, tabv, tok, wst, w1, wqv, bwv, w2, kiv, viv, ccv, csv, ow, inv_s, cos_s, sin_s, raw, qs, qc, gt,
    kvb, full1, full2, full3, inb, outb, fwd, own, sums, vtc, acc, mrow, ocmp, mix, hr, res, part_s,
    l_sem, a_send, a_recv, af_send, af_recv, s_send, s_recv, b_send, b_recv, f_send, f_recv, t_send, t_recv, o_sem,
):
    full = (kvb, full1, full2, full3)
    tp = lax.axis_index("tp")
    kv = lax.axis_index("kv")
    core = lax.rem(tp, 2)
    yy = tp // 2
    zz = kv // 4
    xx = lax.rem(kv, 4)
    sa = 4 - 3 * core
    sb = 1 + 3 * core
    aa = zz * (1 - core) + xx * core
    bb = xx * (1 - core) + zz * core

    def at(r, s):
        return lax.rem(aa + r, 4) * sa + lax.rem(bb + s, 4) * sb

    def tp_at(dy, dc):
        return 2 * lax.rem(yy + dy, 4) + (core + dc - 2 * core * dc)

    def near(r, s):
        return {"kv": at(r, s), "tp": tp}

    local = []

    def fetch(src, dst):
        copy = pltpu.make_async_copy(src, dst, l_sem.at[len(local)])
        copy.start()
        local.append(copy)
        return copy

    w_in = [fetch(h, wst.at[pl.ds(64 * k, 64)]) for k, h in enumerate((wsk_hbm, wsv_hbm, wck_hbm, wcv_hbm))]
    tiles = TOK // TILE

    def tok_in(t):
        return fetch(tok_hbm.at[pl.ds(t * TILE, TILE)], tok.at[pl.ds(t * TILE, TILE)])

    t_in = [tok_in(0)]
    base = pl.ds(pl.multiple_of(kv * 32, 32), 32)
    a_in = [fetch(cc_hbm.at[base], ccv), fetch(cs_hbm.at[base], csv)]
    t_in += [tok_in(1), tok_in(2), tok_in(3)]
    q_in = [fetch(wq_hbm, wqv), fetch(bw_hbm, bwv)]
    i_in = [fetch(ki_hbm, kiv), fetch(vi_hbm, viv)]
    ow_in = fetch(ow_hbm, ow)

    barrier = pltpu.get_barrier_semaphore()
    peers = [near(r, 0) for r in (1, 2, 3)] + [near(0, s) for s in (1, 2, 3)]
    peers += [{"kv": kv, "tp": tp_at(*o)} for o in ORDER[:-1]]
    for peer in peers:
        pl.semaphore_signal(barrier, inc=1, device_id=peer, device_id_type=MESH)

    started = []

    def remote(src, dst, ssem, rsem, dev):
        return pltpu.make_async_remote_copy(
            src_ref=src, dst_ref=dst, send_sem=ssem, recv_sem=rsem, device_id=dev, device_id_type=MESH
        )

    def go(copy):
        copy.start()
        started.append(copy)

    half = NB // 2

    def a_copy(slot, part, r):
        rows = pl.ds(part * half, half)
        i = (slot // 2) * 2 + part
        return remote(kvb.at[rows], full[slot].at[rows], a_send.at[i], a_recv.at[i], near(r, 0))

    def af_copy(slot, part, r):
        rows = pl.ds(part * half, half)
        return remote(full[slot].at[rows], full2.at[rows], af_send.at[part], af_recv.at[part], near(r, 0))

    picks = picks_ref[...]
    code = (picks & (NB - 1)) + jnp.where(picks < 2 * lanes((8, 256)), 64, 0)
    for span in range(16):
        tabv[span:span + 1, :] = jnp.sum(jnp.where((picks >> 5) == span, code, 0), axis=0, keepdims=True)
    tab_in = fetch(tabv, tab)

    gain = gain_ref[...].astype(F32).reshape(1, D)
    for copy in w_in:
        copy.wait()
    for k in range(0, 256, 64):
        w1[k:k + 64, :] = (wst[k:k + 64, :].astype(F32) * gain).astype(BF)
    low = lanes((QB, 128)) < HD
    low64 = lanes((64, 128)) < HD
    front = (lanes((QB, 128)) % 64) < 32

    def turn(v, rows):
        other = jnp.where(front, pltpu.roll(v, 96, 1), pltpu.roll(v, 32, 1))
        return v * cos_s[rows, :] + other * sin_s[rows, :]

    embed = jnp.concatenate([ke_ref[...], ve_ref[...]], axis=1).astype(F32)
    embed = jnp.concatenate([embed] * (QB // CMP), axis=0)
    for t in range(tiles):
        t_in[t].wait()
        if t == 0:
            for copy in a_in:
                copy.wait()
        rows = pl.ds(t * TILE, TILE)
        x = tok[rows, :]
        proj = lax.dot_general(x, w1[...], NT, preferred_element_type=F32)
        xf = x.astype(F32)
        inv = lax.rsqrt(jnp.mean(xf * xf, axis=1, keepdims=True) + EPS)
        inv = jnp.broadcast_to(inv, (TILE, 128))
        inv_s[rows, :] = inv
        for j in range(TILE // QB):
            part = pl.ds(t * TILE + j * QB, QB)
            for u in (0, 1):
                g = t * (TILE // 64) + 2 * j + u
                cc, cs = ccv[g:g + 1, :], csv[g:g + 1, :]
                cos_s[pl.ds(g * 64, 64), :] = cc * fc_ref[...] - cs * fs_ref[...]
                sin_s[pl.ds(g * 64, 64), :] = (cs * fc_ref[...] + cc * fs_ref[...]) * sg_ref[...]
            scale = inv[j * QB:(j + 1) * QB]
            sel = proj[j * QB:(j + 1) * QB, 0:128] * scale
            sel = jnp.where(low, turn(sel, part), sel)
            vt = sel.T[64:128]
            b = t * (TILE // SEL) + 2 * j
            kvb[b] = jnp.where(low64, sel[0:64], pltpu.roll(vt, 64, 1)).astype(BF)
            kvb[b + 1] = jnp.where(low64, sel[64:128], vt).astype(BF)
            val = (proj[j * QB:(j + 1) * QB, 128:256] * scale).astype(BF).astype(F32) + embed
            val = val.astype(BF).astype(F32)
            for n in range(QB // CMP):
                spot = (t * (TILE // CMP) + j * (QB // CMP) + n) * PITCH
                raw[spot:spot + CMP, :] = val[n * CMP:(n + 1) * CMP]
        if t % 2 == 1:
            if t == 1:
                pl.semaphore_wait(barrier, len(peers))
            for slot, r in ((3, 1), (1, 3)):
                go(a_copy(slot, t // 2, r))

    def dest_of(c):
        dest = 0
        for k in range(8):
            dest = dest + jnp.where(c == k, tp_at(*ORDER[k]), 0)
        return dest

    def select(r, g):
        span = at(r, 0)
        dests = [at(0, s) for s in range(4)]

        def body(c, _):
            q0 = dest_of(c) * 2
            for k in (0, 1):
                for s in range(4):
                    blk = tab[span, dests[s] * 16 + q0 + k] & (NB - 1)
                    val = full[r][blk]
                    if s == 0:
                        inb[r, 0, 2 * c + k] = val
                    else:
                        outb[r, s - 1, 2 * c + k] = val
            return 0

        lax.fori_loop(4 * g, 4 * g + 4, body, 0)

    def f_copy(r, g, k):
        part = pl.ds(8 * g + 4 * k, 4)
        return remote(
            outb.at[r, 1, part], fwd.at[r, g, k], f_send.at[r, 2 * g + k], f_recv.at[r, 2 * g + k],
            near(0, 1 + 2 * k),
        )

    def b_copy(r, g, k):
        part = pl.ds(8 * g, 8)
        return remote(
            outb.at[r, 2 * k, part], inb.at[r, 3 - 2 * k, part], b_send.at[r, g, k], b_recv.at[r, g, k],
            near(0, 1 + 2 * k),
        )

    def bf_copy(r, g, k):
        part = pl.ds(8 * g + 4 * k, 4)
        return remote(
            fwd.at[r, g, k], inb.at[r, 2, part], b_send.at[r, g, 2 + k], b_recv.at[r, g, 2 + k],
            near(0, 1 + 2 * k),
        )

    def f_start(r, g):
        for k in (0, 1):
            go(f_copy(r, g, k))

    def d_start(r, g):
        for k in (0, 1):
            go(b_copy(r, g, k))

    def b_start(r, g):
        f_start(r, g)
        d_start(r, g)

    def b_forward(r, g):
        for k in (0, 1):
            f_copy(r, g, k).wait_recv()
            go(bf_copy(r, g, k))

    def b_wait(r, g):
        for k in (0, 1):
            b_copy(r, g, k).wait_recv()
            bf_copy(r, g, k).wait_recv()

    tab_in.wait()
    for g in (0, 1):
        select(0, g)
        f_start(0, g)
    d_start(0, 0)
    d_start(0, 1)

    for copy in i_in:
        copy.wait()
    keys, values = [], []
    for r in range(0, CMP, 2):
        one = raw[pl.ds(r, 64, stride=PITCH), :]
        two = raw[pl.ds(r + 1, 64, stride=PITCH), :]
        keys.append(jnp.where(low64, one, pltpu.roll(two, 64, 1)).astype(BF))
        values.append(jnp.where(low64, pltpu.roll(one, 64, 1), two).astype(BF))
    parts = []
    for rows, inner, outer in ((keys, kiv, ko_ref), (values, viv, vo_ref)):
        flat = jnp.concatenate(rows, axis=1)
        hidden = gelu(lax.dot_general(flat, inner[...], NT, preferred_element_type=F32)).astype(BF)
        parts.append(jnp.dot(hidden, outer[...], preferred_element_type=F32))
    both = jnp.concatenate(parts, axis=1)
    own[...] = jnp.where(low64, both, jnp.concatenate([both, both], axis=0).T[64:128]).astype(BF)
    sums[0, 0] = own[...]

    def s_copy(r):
        return remote(own, sums.at[0, 4 - r], s_send.at[r - 1], s_recv.at[3 - r], near(r, 0))

    def s_bundle(s):
        return remote(sums.at[0], sums.at[4 - s], s_send.at[2 + s], s_recv.at[6 - s], near(0, s))

    for r in (1, 2, 3):
        go(s_copy(r))

    a_copy(3, 0, 1).wait_recv()
    go(af_copy(3, 0, 1))

    for copy in q_in:
        copy.wait()
    w2[0:128, :] = (wqv[...].T.astype(F32) * gain).astype(BF)
    row = rows_of((128, 16))
    col = lanes((128, 16))
    e0 = jnp.where((row < 2) & (col == 2 * tp + row), 1.0, 0.0).astype(BF)
    e1 = jnp.where((row >= 2) & (row < 4) & (col == 2 * tp + row - 2), 1.0, 0.0).astype(BF)
    picked = jnp.dot(e0, bwv[0], preferred_element_type=F32) + jnp.dot(e1, bwv[1], preferred_element_type=F32)
    w2[128:256, :] = (picked * gain).astype(BF)
    zero = jnp.zeros((64, 256), BF)

    def queries(t):
        rows = pl.ds(t * TILE, TILE)
        proj = lax.dot_general(tok[rows, :], w2[...], NT, preferred_element_type=F32)
        for j in range(TILE // QB):
            part = pl.ds(t * TILE + j * QB, QB)
            q = t * (TILE // QB) + j
            scale = inv_s[part, :]
            v = proj[j * QB:(j + 1) * QB, 0:128] * scale
            for ref, val in ((qc, v), (qs, turn(v, part))):
                val = (val.T.astype(BF).astype(F32) * 0.125).astype(BF)
                ref[q, 0:64, 0:128] = val[0:64]
                ref[q, 0:64, 128:256] = val[64:128]
                ref[q, 64:128, :] = zero
            g = proj[j * QB:(j + 1) * QB, 128:256] * scale
            gt[q] = 1.0 / (1.0 + jnp.exp(-g.T[0:8]))

    queries(0)
    queries(1)
    a_copy(1, 1, 1).wait_recv()
    go(af_copy(1, 1, 3))
    for r in (1, 2, 3):
        s_copy(r).wait_recv()
    for s in (1, 2, 3):
        go(s_bundle(s))
    queries(2)
    queries(3)
    b_forward(0, 0)
    b_forward(0, 1)
    a_copy(3, 1, 1).wait_recv()
    a_copy(1, 0, 1).wait_recv()
    for g in (0, 1):
        for r in (3, 1):
            select(r, g)
            f_start(r, g)
    d_start(3, 0)
    d_start(1, 0)

    def values_of(blocks):
        pairs = [
            jnp.concatenate([blocks[k][:, HD:], blocks[k + 1][:, HD:]], axis=1) for k in range(0, len(blocks), 2)
        ]
        vt = jnp.concatenate(pairs, axis=1)
        return jnp.concatenate([vt, jnp.ones((16, vt.shape[1]), BF)], axis=0)

    def top(s):
        return jnp.max(s, axis=0, keepdims=True)

    def own_group(g):
        ids = [(tp_at(*ORDER[c]) * 2 + k, 2 * c + k) for c in range(4 * g, 4 * g + 4) for k in (0, 1)]
        blocks = [[kvb[2 * q], kvb[2 * q + 1]] for q, _ in ids]
        scs = [
            jnp.dot(jnp.concatenate(blk, axis=0), qs[q], preferred_element_type=F32)
            for blk, (q, _) in zip(blocks, ids)
        ]
        ps = []
        for sc, (_, i) in zip(scs, ids):
            sc = jnp.where(rows_of(sc.shape) <= (lanes(sc.shape) & (QB - 1)), sc, NEG)
            m = top(sc)
            mrow[i] = m
            ps.append(jnp.exp(sc - m).astype(BF))
        for p, blk, (_, i) in zip(ps, blocks, ids):
            acc[i] = jnp.dot(values_of(blk), p, preferred_element_type=F32)

    def far_steps(ids, r):
        blocks = [[inb[r, s, i] for s in range(4)] for _, i in ids]
        scs = [
            jnp.dot(jnp.concatenate(blk, axis=0), qs[q], preferred_element_type=F32)
            for blk, (q, _) in zip(blocks, ids)
        ]
        ms, ps, scale = [], [], []
        for sc, (q, i) in zip(scs, ids):
            m = old = mrow[i]
            bias = []
            for s in range(4):
                used = lax.shift_right_logical(tab[at(r, s), kv * 16 + q], 6)
                bias.append((used.astype(F32) - 1.0) * 1e30)
                m = jnp.maximum(m, top(sc[64 * s:64 * s + 64]) + bias[s])
            p = [jnp.exp(sc[64 * s:64 * s + 64] - (m - bias[s])).astype(BF) for s in range(4)]
            ms.append(m)
            ps.append(jnp.concatenate(p, axis=0))
            scale.append(jnp.exp(old - m))
        adds = [jnp.dot(values_of(blk), p, preferred_element_type=F32) for blk, p in zip(blocks, ps)]
        return ms, [acc[i] * sc + add for (_, i), sc, add in zip(ids, scale, adds)]

    def ids_of(c0, n):
        return [(tp_at(*ORDER[c]) * 2 + k, 2 * c + k) for c in range(c0, c0 + n) for k in (0, 1)]

    def far_loop(g, lo, hi):
        ids = ids_of(4 * g, 4)

        def body(n, _):
            ms, accs = far_steps(ids, n + n // 2)
            for (_, i), m, a in zip(ids, ms, accs):
                mrow[i] = m
                acc[i] = a
            return 0

        lax.fori_loop(lo, hi, body, 0)

    def compressed(n, _):
        ids = []
        for c in (n,):
            q0 = dest_of(c) * 2
            ids += [(q0 + k, 2 * c + k) for k in (0, 1)]
        scs = [
            [jnp.dot(sums[s].reshape(256, 128), qc[q], preferred_element_type=F32) for s in range(4)] for q, _ in ids
        ]
        ps = []
        for (q, _), sc in zip(ids, scs):
            ones, ms = [], []
            m = jnp.full((1, 256), FLOOR, F32)
            for s in range(4):
                for r in range(4):
                    one = sc[s][64 * r:64 * r + 64]
                    bias = jnp.where(at(r, s) < kv, 0.0, NEG)
                    if r == 0 and s == 0:
                        end = (rows_of(one.shape) + 1) * CMP - 1
                        one = jnp.where(end <= q * QB + (lanes(one.shape) & (QB - 1)), one, NEG)
                        bias = 0.0
                    ones.append(one)
                    ms.append(bias)
                    m = jnp.maximum(m, top(one) + bias)
            ps.append(jnp.concatenate([jnp.exp(o - (m - b)).astype(BF) for o, b in zip(ones, ms)], axis=0))
        for (_, i), p in zip(ids, ps):
            total = jnp.dot(vtc[...], p, preferred_element_type=F32)
            den = total[64:65]
            ocmp[i] = jnp.where(den > 0, total[0:64] / jnp.maximum(den, 1e-30), 0.0)
        return 0

    def finish(c0, n):
        ids = ids_of(c0, n)
        _, accs = far_steps(ids, 2)
        for (q, i), a in zip(ids, accs):
            o = a[0:64] / a[64:65]
            oc = ocmp[i]
            g = gt[q]
            heads = [
                g[h:h + 1] * oc[:, 128 * h:128 * h + 128] + g[2 + h:3 + h] * o[:, 128 * h:128 * h + 128]
                for h in (0, 1)
            ]
            mix[i // 2, (i % 2) * QB:(i % 2 + 1) * QB, :] = jnp.concatenate(heads, axis=0).T.astype(BF)

    def t_copy(c, slot):
        return remote(mix.at[c], hr.at[slot], t_send.at[c], t_recv.at[c], {"kv": kv, "tp": tp_at(*ORDER[c])})

    own_group(0)
    own_group(1)
    af_copy(3, 0, 1).wait_recv()
    af_copy(1, 1, 1).wait_recv()
    for g in (0, 1):
        select(2, g)
        f_start(2, g)
    b_forward(3, 0)
    b_forward(1, 0)
    d_start(2, 0)
    for s in (1, 2, 3):
        s_bundle(s).wait_recv()
    for s in range(4):
        vtc[:, 256 * s:256 * s + 256] = values_of([sums[s, r] for r in range(4)])
    lax.fori_loop(0, 4, compressed, 0)
    b_forward(2, 0)
    b_forward(3, 1)
    b_forward(1, 1)
    for r in (3, 1, 2):
        d_start(r, 1)
    lax.fori_loop(4, 6, compressed, 0)
    b_forward(2, 1)
    lax.fori_loop(6, 8, compressed, 0)
    for g in (0, 1):
        b_wait(0, g)
        far_loop(g, 0, 1)
    for g in (0, 1):
        for r in (3, 1):
            b_wait(r, g)
        far_loop(g, 1, 3)
        b_wait(2, g)
        for c in (4 * g, 4 * g + 2):
            finish(c, 2)
            for k in (c, c + 1):
                if k < 7:
                    go(t_copy(k, tp))
    hr[tp] = mix[7]

    ow_in.wait()

    def source(c):
        dy, dc = ORDER[c]
        return tp_at((4 - dy) % 4, dc)

    def arrive(c):
        t_copy(c, source(c)).wait_recv()

    def product(cs, cols):
        x = jnp.concatenate([hr[source(c)] for c in cs], axis=1)
        w = jnp.concatenate([ow[pl.ds(pl.multiple_of(source(c) * 128, 128), 128), cols] for c in cs], axis=0)
        return jnp.dot(x, w, preferred_element_type=F32)

    early, late = (7, 0, 1, 2, 3), (4, 5, 6)
    for c in early[1:]:
        arrive(c)
    for n in range(4):
        cols = pl.ds(n * 512, 512)
        part_s[:, cols] = product(early, cols)
    for c in late:
        arrive(c)
    outs = []
    for n in range(4):
        cols = pl.ds(n * 512, 512)
        res[:, cols] = (part_s[:, cols] + product(late, cols)).astype(BF)
        copy = pltpu.make_async_copy(res.at[:, cols], out_hbm.at[:, cols], o_sem.at[n])
        copy.start()
        outs.append(copy)
    for copy in started:
        copy.wait_send()
    for copy in outs:
        copy.wait()


def per_device(
    tokens, norm_gain, query_weight, cmp_key_weight, cmp_value_weight, sel_key_weight, sel_value_weight,
    branch_weight, key_embed, key_inner, key_outer, value_embed, value_inner, value_outer, out_weight, chosen,
):
    cc, cs, fc, fs, sg = angle_tables()
    vm = pl.BlockSpec(memory_space=pltpu.VMEM)
    hbm = pl.BlockSpec(memory_space=pl.ANY)
    dma = pltpu.SemaphoreType.DMA
    v = pltpu.VMEM
    return pl.pallas_call(
        kernel,
        in_specs=[vm] * 9 + [hbm] * 12,
        out_specs=hbm,
        out_shape=jax.ShapeDtypeStruct((256, D), BF),
        scratch_shapes=[
            pltpu.SMEM((16, 256), jnp.int32), v((16, 256), jnp.int32),
            v((TOK, D), BF), v((256, D), BF), v((256, D), BF), v((D, 128), BF), v((2, 16, D), BF), v((256, D), BF),
            v((64, D), BF), v((64, D), BF), v((32, 128), F32), v((32, 128), F32), v((1024, D), BF),
            v((TOK, 128), F32), v((TOK, 128), F32), v((TOK, 128), F32), v((64 * PITCH, 128), F32),
            v((NQ, 128, 256), BF), v((NQ, 128, 256), BF), v((NQ, 8, 128), F32),
            v((NB, SEL, 128), BF), v((NB, SEL, 128), BF), v((NB, SEL, 128), BF), v((NB, SEL, 128), BF),
            v((4, 4, NQ, SEL, 128), BF), v((4, 3, NQ, SEL, 128), BF), v((4, 2, 2, 4, SEL, 128), BF),
            v((64, 128), BF), v((4, 4, 64, 128), BF), v((80, 1024), BF),
            v((NQ, 80, 256), F32), v((NQ, 1, 256), F32), v((NQ, 64, 256), F32),
            v((8, 256, 128), BF), v((8, 256, 128), BF), v((256, D), BF), v((256, D), F32),
            dma((17,)), dma((4,)), dma((4,)), dma((2,)), dma((2,)), dma((6,)), dma((6,)),
            dma((4, 2, 4)), dma((4, 2, 4)), dma((4, 4)), dma((4, 4)), dma((8,)), dma((8,)), dma((4,)),
        ],
        compiler_params=pltpu.CompilerParams(collective_id=0, has_side_effects=True, vmem_limit_bytes=67043328),
        name="layer",
    )(
        chosen[0].T, norm_gain, key_embed[0], key_outer[0], value_embed[0], value_outer[0], fc, fs, sg,
        tokens, query_weight, cmp_key_weight.T, cmp_value_weight.T, sel_key_weight.T, sel_value_weight.T,
        branch_weight.transpose(0, 2, 1), key_inner[0].T, value_inner[0].T, cc, cs, out_weight,
    )


def solution(mesh):
    placed = (
        P("kv", None), P(), P(None, "tp"), P(None, "tp"), P(None, "tp"), P(None, "tp"), P(None, "tp"), P(),
        P("tp", None, None), P("tp", None, None), P("tp", None, None), P("tp", None, None),
        P("tp", None, None), P("tp", None, None), P(), P("tp", None, None),
    )
    return jax.shard_map(
        per_device, mesh=mesh, in_specs=placed, out_specs=P(("kv", "tp"), None), check_vma=False
    )
```
